256 devices in a mesh: sp: 64 (over z, y, core), tp: 4 (over x).
Axes of the slice: x: 4, y: 4, z: 8, core: 2. Of those that a mesh axis runs over, the one named last changes fastest.
Arguments:
- stream: bfloat16 [8192, 2048], P('sp', 'tp'), may hold values from -40 to 40
- queries: bfloat16 [8192, 1024], P('sp', 'tp'), may hold values from -6 to 6
- keys: bfloat16 [8192, 1024], P('sp', 'tp'), may hold values from -6 to 6
- values: bfloat16 [8192, 2048], P('sp', 'tp'), may hold values from -25 to 25
- out_gate: bfloat16 [8192, 2048], P('sp', 'tp'), may hold values from -8 to 8
- input_gate: float32 [8192, 8], P('sp', 'tp'), may hold values from -9 to 350
- forget_gate: float32 [8192, 8], P('sp', 'tp'), may hold values from -4 to 20
- head_gain: float32 [2048], P('tp'), may hold values from 0.1 to 1.9
- w_out: bfloat16 [2048, 2048], P('tp'), may hold values from -0.125 to 0.125
- ffn_gain: float32 [2048], replicated, may hold values from 0.1 to 1.9
- w_gate: bfloat16 [2048, 5632], P('sp', 'tp'), may hold values from -0.125 to 0.125
- w_up: bfloat16 [2048, 5632], P('sp', 'tp'), may hold values from -0.125 to 0.125
- w_down: bfloat16 [5632, 2048], P('tp', 'sp'), may hold values from -0.078125 to 0.078125
Outputs:
- mixed: bfloat16 [8192, 2048], P('sp', 'tp')
The draws below stay inside these ranges and needn't reach their ends.
All inputs are finite; a program needn't handle non-finite values.
Results may differ from the reference program's by a relative error of at most 0.0095.
Values may be sent and summed in bfloat16 or wider, within the bound.
A program may use at most 128 MiB of HBM per device.

```python
import math
import jax
import jax.numpy as jnp
from jax import lax

D = 2048
HEADS = 8
DQK = 128
DV = 256
FF = 5632
BLOCK = 64
TOK_DEV = 128
SEQUENCE_TOKENS = 8192
VALS = 2048
N_SP = 64
N_TP = 4


def draw_stream(key, part):
    first, second = jax.random.split(jax.random.fold_in(key, 11), 2)
    rising = 3.0 ** (jnp.arange(D, dtype=jnp.float32) / D)
    rough = jnp.exp(jax.random.uniform(second, (D,), jnp.float32, -0.5, 0.5))
    full = jnp.clip(jax.random.normal(first, (SEQUENCE_TOKENS, D), jnp.float32), -5.0, 5.0) * rising * rough
    return full.astype(jnp.bfloat16)


def draw_values(key, part):
    first, second = jax.random.split(jax.random.fold_in(key, 41), 2)
    head_place = (jnp.arange(VALS) // DV).astype(jnp.float32)
    rising = 3.0 ** (head_place / (HEADS - 1))
    rough = jnp.exp(jax.random.uniform(second, (VALS,), jnp.float32, -0.5, 0.5))
    base = jnp.clip(jax.random.normal(first, (SEQUENCE_TOKENS, VALS), jnp.float32), -5.0, 5.0)
    return (base * rising * rough).astype(jnp.bfloat16)


def draw_input_gate(key, part):
    first = jax.random.fold_in(jax.random.fold_in(key, 23), 0)
    base = jnp.clip(1.5 * jax.random.normal(first, (SEQUENCE_TOKENS, HEADS), jnp.float32), -9.0, 9.0)
    return base


def draw_forget_gate(key, part):
    partition_key = jax.random.split(jax.random.fold_in(key, 37), 6)
    fast_share = 0.5
    fast = jax.random.uniform(partition_key[0], (HEADS,), jnp.float32) < fast_share
    fast_rate = 1.0 / jax.random.uniform(partition_key[1], (HEADS,), jnp.float32, 30.0, 100.0)
    slow_rate = 0.12 * math.log(10.0) / SEQUENCE_TOKENS
    factor = jnp.exp(jax.random.uniform(partition_key[2], (SEQUENCE_TOKENS // TOK_DEV, 1), jnp.float32, -math.log(2.0), math.log(2.0)))
    factor = jnp.repeat(factor, TOK_DEV, axis=0)
    speed_ratio = jnp.where(fast, fast_rate, slow_rate)[None, :] * factor
    position_slots = jax.random.randint(partition_key[3], (3,), 0, SEQUENCE_TOKENS)
    spike_events = jnp.any(jnp.arange(SEQUENCE_TOKENS)[:, None] == position_slots[None, :], axis=1)[:, None]
    spike_frequency = -jnp.log(jax.random.uniform(partition_key[4], (SEQUENCE_TOKENS, 1), jnp.float32, 0.55, 0.8))
    speed_ratio = jnp.where(spike_events, spike_frequency, speed_ratio)
    noise = jnp.clip(0.7 * jax.random.normal(partition_key[5], (SEQUENCE_TOKENS, HEADS), jnp.float32), -2.0, 2.0)
    return -jnp.log(jnp.expm1(speed_ratio)) + noise


def block_levels(key, dims, cuts, least, top_value):
    loudness, own = 1.0, jax.random.fold_in(key, 6)
    for axis_at, blocks in cuts:
        heights = jnp.exp(jax.random.uniform(jax.random.fold_in(own, axis_at), (blocks,), jnp.float32, least / len(cuts), top_value / len(cuts)))
        loudness = loudness * jnp.repeat(heights, dims[axis_at] // blocks).reshape([-1 if axis == axis_at else 1 for axis in range(len(dims))])
    return loudness


def normal_values(rng, dims, scale, reach, shards=(), kind=jnp.bfloat16):
    drawn = scale * jax.random.normal(rng, dims, jnp.float32)
    if shards:
        drawn = drawn * block_levels(rng, dims, shards, -0.22, 0.18)
    return jnp.clip(drawn, -reach, reach).astype(kind)


def setup_inputs(seed: int = 0) -> dict:
    seeds = jax.random.split(jax.random.key(seed), 14)
    return {
        "stream": draw_stream(jax.random.fold_in(seeds[13], 71), 0),
        "queries": normal_values(seeds[1], (SEQUENCE_TOKENS, HEADS * DQK), 1.0, 6.0, ((0, 64), (1, 4))),
        "keys": normal_values(seeds[2], (SEQUENCE_TOKENS, HEADS * DQK), 1.0, 6.0, ((0, 64), (1, 4))),
        "values": draw_values(jax.random.fold_in(seeds[13], 71), 0),
        "out_gate": normal_values(seeds[4], (SEQUENCE_TOKENS, VALS), 1.5, 8.0, ((0, 64), (1, 4))),
        "input_gate": draw_input_gate(jax.random.fold_in(seeds[13], 71), 0),
        "forget_gate": draw_forget_gate(jax.random.fold_in(seeds[13], 71), 0),
        "head_gain": jnp.clip(1.0 + 0.18 * jax.random.normal(seeds[7], (VALS,), jnp.float32), 0.1, 1.9),
        "w_out": normal_values(seeds[8], (VALS, D), VALS ** -0.5, 0.125, ((0, 4),)),
        "ffn_gain": jnp.clip(1.0 + 0.18 * jax.random.normal(seeds[9], (D,), jnp.float32), 0.1, 1.9),
        "w_gate": normal_values(seeds[10], (D, FF), D ** -0.5, 0.125, ((0, 64), (1, 4))),
        "w_up": normal_values(seeds[11], (D, FF), D ** -0.5, 0.125, ((0, 64), (1, 4))),
        "w_down": normal_values(seeds[12], (FF, D), FF ** -0.5, 0.078125, ((0, 4), (1, 64))),
    }


precise = lax.Precision.HIGHEST
norm_eps = 1e-06
very_low = -1e+30

def block_summary(key_blk, value_blk, input_blk, decay_sum):
    decay_total = decay_sum[..., -1]
    log_weight = decay_total[..., None] - decay_sum + input_blk
    weight_peak = lax.optimization_barrier(jnp.max(log_weight, axis=-1))
    weights = jnp.exp(log_weight - weight_peak[..., None])
    state_mat = jnp.einsum('...ld,...le->...de', weights[..., None] * key_blk, value_blk, precision=precise)
    state_vec = jnp.einsum('...l,...ld->...d', weights, key_blk, precision=precise)
    return (state_mat, state_vec, weight_peak, decay_total)

def combine(earlier, later):
    ceiling = jnp.maximum(later[3] + earlier[2], later[2])
    former = jnp.exp(later[3] + earlier[2] - ceiling)
    latter = jnp.exp(later[2] - ceiling)
    return (former[..., None, None] * earlier[0] + latter[..., None, None] * later[0], former[..., None] * earlier[1] + latter[..., None] * later[1], ceiling, earlier[3] + later[3])

def block_output(query_blk, key_blk, value_blk, input_blk, decay_sum, state_mat, state_vec, state_peak):
    block_len = query_blk.shape[-2]
    causal = jnp.tril(jnp.ones((block_len, block_len), jnp.bool_))
    log_pair = jnp.where(causal, decay_sum[..., :, None] - decay_sum[..., None, :] + input_blk[..., None, :], -jnp.inf)
    log_carry = decay_sum + state_peak[..., None]
    row_peak = jnp.maximum(log_carry, lax.optimization_barrier(jnp.max(log_pair, axis=-1)))
    scores = jnp.einsum('...ld,...sd->...ls', query_blk, key_blk, precision=precise) * jnp.exp(log_pair - row_peak[..., None])
    carried = jnp.exp(log_carry - row_peak)
    numer = jnp.einsum('...ls,...se->...le', scores, value_blk, precision=precise) + carried[..., None] * jnp.einsum('...ld,...de->...le', query_blk, state_mat, precision=precise)
    normer = lax.optimization_barrier(jnp.sum(scores, axis=-1)) + carried * jnp.einsum('...ld,...d->...l', query_blk, state_vec, precision=precise)
    denom = jnp.maximum(jnp.abs(normer), jnp.exp(-row_peak))
    return numer / denom[..., None]

def reference(stream, queries, keys, values, out_gate, input_gate, forget_gate, head_gain, w_out, ffn_gain, w_gate, w_up, w_down):
    blocks = SEQUENCE_TOKENS // BLOCK

    def to_blocks(array, col_width):
        return array.reshape(blocks, BLOCK, HEADS, col_width).transpose(0, 2, 1, 3)
    query_all = to_blocks(queries, DQK)
    key_all = to_blocks(keys, DQK)
    value_all = to_blocks(values, DV)
    input_all = input_gate.reshape(blocks, BLOCK, HEADS).transpose(0, 2, 1)
    forget_all = forget_gate.reshape(blocks, BLOCK, HEADS).transpose(0, 2, 1)

    def advance(carry, pieces):
        query_blk = pieces[0].astype(jnp.float32) * DQK ** (-0.5)
        key_blk = pieces[1].astype(jnp.float32)
        value_blk = pieces[2].astype(jnp.float32)
        decay_sum = jnp.cumsum(jax.nn.log_sigmoid(pieces[4]), axis=-1)
        output = block_output(query_blk, key_blk, value_blk, pieces[3], decay_sum, carry[0], carry[1], carry[2])
        return (combine(carry, block_summary(key_blk, value_blk, pieces[3], decay_sum)), output)
    start = (jnp.zeros((HEADS, DQK, DV), jnp.float32), jnp.zeros((HEADS, DQK), jnp.float32), jnp.full((HEADS,), very_low, jnp.float32), jnp.zeros((HEADS,), jnp.float32))
    _, mixed_heads = lax.scan(advance, start, (query_all, key_all, value_all, input_all, forget_all))
    head_rows = mixed_heads.transpose(0, 2, 1, 3).reshape(SEQUENCE_TOKENS, HEADS, DV)
    mean_sq = lax.optimization_barrier(jnp.mean(head_rows * head_rows, axis=(1, 2), keepdims=True))
    gated = head_rows * lax.rsqrt(mean_sq + norm_eps) * head_gain.reshape(HEADS, DV) * jax.nn.sigmoid(out_gate.astype(jnp.float32).reshape(SEQUENCE_TOKENS, HEADS, DV))
    heads_out = gated.reshape(SEQUENCE_TOKENS, HEADS * DV).astype(jnp.bfloat16)
    group = HEADS * DV // N_TP
    mixer = jnp.zeros((SEQUENCE_TOKENS, D), jnp.float32)
    for member in range(N_TP):
        partial_value = jnp.dot(heads_out[:, member * group:(member + 1) * group], w_out[member * group:(member + 1) * group], preferred_element_type=jnp.float32).astype(jnp.bfloat16)
        mixer = mixer + lax.optimization_barrier(partial_value).astype(jnp.float32)
    resid = (stream.astype(jnp.float32) + mixer).astype(jnp.bfloat16)
    hidden_group = FF // N_TP

    def channel_mix(rows_in):
        rows_float = rows_in.astype(jnp.float32)
        normed = (rows_float * lax.rsqrt(lax.optimization_barrier(jnp.mean(rows_float * rows_float, axis=-1, keepdims=True)) + norm_eps) * ffn_gain).astype(jnp.bfloat16)
        gate_act = jnp.dot(normed, w_gate, preferred_element_type=jnp.float32)
        up_act = jnp.dot(normed, w_up, preferred_element_type=jnp.float32)
        hidden = (jax.nn.silu(gate_act) * up_act).astype(jnp.bfloat16)
        totals = jnp.zeros((rows_in.shape[0], D), jnp.float32)
        for member in range(N_TP):
            partial_value = jnp.dot(hidden[:, member * hidden_group:(member + 1) * hidden_group], w_down[member * hidden_group:(member + 1) * hidden_group], preferred_element_type=jnp.float32).astype(jnp.bfloat16)
            totals = totals + lax.optimization_barrier(partial_value).astype(jnp.float32)
        return (rows_float + totals).astype(jnp.bfloat16)
    mixed = lax.map(channel_mix, resid.reshape(N_SP, TOK_DEV, D))
    return mixed.reshape(SEQUENCE_TOKENS, D)
```

```python
import functools

import jax
import jax.numpy as jnp
from jax import lax
from jax.experimental import pallas as pl
from jax.experimental.pallas import tpu as pltpu
from jax.sharding import PartitionSpec as P

D = 2048
DQK = 128
DV = 256
VALS = 2048
FFT = 1408
TOK = 128
COLS = 512
NG = 8
NZ = 8
NX = 4
norm_eps = 1e-06
very_low = -1e30
MESH = pl.DeviceIdType.MESH
f32 = jnp.float32
bf16 = jnp.bfloat16


def row_of(col, eye):
    return jnp.sum(jnp.where(eye, col, 0.0), axis=0, keepdims=True)


def col_of(row, eye):
    return jnp.sum(jnp.where(eye, row, 0.0), axis=1, keepdims=True)


def split_hi_lo(x):
    hi = x.astype(bf16)
    return hi, (x - hi.astype(f32)).astype(bf16)


def dot(a, b, dims=((1,), (0,))):
    return lax.dot_general(a, b, (dims, ((), ())), preferred_element_type=f32)


def log_sigmoid(x):
    return jnp.minimum(x, 0.0) - jnp.log1p(jnp.exp(-jnp.abs(x)))


def copy_to(src, dst, ssem, rsem, dev):
    return pltpu.make_async_remote_copy(
        src_ref=src, dst_ref=dst, send_sem=ssem, recv_sem=rsem, device_id=dev, device_id_type=MESH
    )


def barrier_all(devs):
    bar = pltpu.get_barrier_semaphore()
    for dev in devs:
        pl.semaphore_signal(bar, inc=1, device_id=dev, device_id_type=MESH)
    return bar, len(devs)


def cell_kernel(
    q_ref,
    k_ref,
    v_ref,
    og_ref,
    ig_ref,
    fg_ref,
    hg_ref,
    wo_ref,
    st_ref,
    gain_ref,
    y_ref,
    r_ref,
    resid_ref,
    small1,
    small2,
    small_l,
    small_me,
    small_t,
    s_loc,
    r1,
    pre_l,
    t_loc,
    r2,
    o3,
    r3,
    part,
    rpart,
    sq_me,
    rsq,
    yloc,
    ss,
    rs,
):
    sp, tp = lax.axis_index("sp"), lax.axis_index("tp")
    z, g = sp // NG, lax.rem(sp, NG)
    gpeer = [lax.rem(g + r, NG) for r in range(NG)]
    gfrom = [lax.rem(g + NG - r, NG) for r in range(NG)]
    zpeer = [lax.rem(z + r, NZ) for r in range(NZ)]
    xpeer = [lax.rem(tp + r, NX) for r in range(NX)]
    xfrom = [lax.rem(tp + NX - r, NX) for r in range(NX)]
    gdev = [{"sp": z * NG + p, "tp": tp} for p in gpeer]
    zdev = [{"sp": p * NG + g, "tp": tp} for p in zpeer]
    xdev = [{"sp": sp, "tp": p} for p in xpeer]
    bar, count = barrier_all(gdev[1:] + zdev[1:] + xdev[1:])

    rows = lax.broadcasted_iota(jnp.int32, (TOK, TOK), 0)
    cols = lax.broadcasted_iota(jnp.int32, (TOK, TOK), 1)
    eye = rows == cols
    low = rows >= cols

    lf = log_sigmoid(fg_ref[...])
    ig = ig_ref[...]
    small_me[...] = jnp.zeros_like(small_me)
    cs_cols, pairs, wks = [], [], []
    for h in range(2):
        lf_col = lf[:, h : h + 1]
        lf_row = row_of(lf_col, eye)
        cs_col = jnp.sum(jnp.where(low, lf_row, 0.0), axis=1, keepdims=True)
        cs_row = jnp.sum(jnp.where(rows <= cols, lf_col, 0.0), axis=0, keepdims=True)
        ig_col = ig[:, h : h + 1]
        ig_row = row_of(ig_col, eye)
        rest_row = ig_row - cs_row
        rest_col = ig_col - cs_col
        top = jnp.max(rest_row, axis=1, keepdims=True)
        total = jnp.sum(lf_row, axis=1, keepdims=True)
        wk = jnp.exp(rest_col - top) * k_ref[:, h * DQK : (h + 1) * DQK].astype(f32)
        small_me[h : h + 1, :] = jnp.sum(wk, axis=0, keepdims=True)
        small_me[2 + h : 3 + h, :] = jnp.broadcast_to(total, (1, TOK))
        small_me[4 + h : 5 + h, :] = jnp.broadcast_to(total + top, (1, TOK))
        cs_cols.append(cs_col)
        pairs.append((rest_row, ig_row))
        wks.append(wk)
    pl.semaphore_wait(bar, count)
    pending = []
    for r in range(1, NG):
        c = copy_to(small_me, small1.at[g], ss.at[0, r], rs.at[0, r], gdev[r])
        c.start()
        pending.append(c)
    small1[g] = small_me[...]

    for h in range(2):
        hi, lo = split_hi_lo(wks[h])
        v_h = v_ref[:, h * DV : (h + 1) * DV]
        state = dot(hi, v_h, ((0,), (0,))) + dot(lo, v_h, ((0,), (0,)))
        s_loc[4 * h : 4 * h + 4] = state.astype(bf16).reshape(4, 32, DV)
    for r in range(1, NG):
        c = copy_to(s_loc.at[gpeer[r]], r1.at[g], ss.at[1, r], rs.at[1, r], gdev[r])
        c.start()
        pending.append(c)
    r1[g] = s_loc[g]

    scale = DQK**-0.5
    num0, den0, peak0 = [], [], []
    for h in range(2):
        rest_row, ig_row = pairs[h]
        q_h = q_ref[:, h * DQK : (h + 1) * DQK]
        k_h = k_ref[:, h * DQK : (h + 1) * DQK]
        log_pair = jnp.where(low, cs_cols[h] + rest_row, -jnp.inf)
        peak = jnp.max(log_pair, axis=1, keepdims=True)
        scores = dot(q_h, k_h, ((1,), (1,))) * scale * jnp.exp(log_pair - peak)
        hi, lo = split_hi_lo(scores)
        v_h = v_ref[:, h * DV : (h + 1) * DV]
        num0.append(dot(hi, v_h) + dot(lo, v_h))
        den0.append(jnp.sum(scores, axis=1, keepdims=True))
        peak0.append(peak)

    for r in range(1, NG):
        pltpu.make_async_remote_copy(
            small_me, small1.at[gfrom[r]], ss.at[0, r], rs.at[0, r], gdev[r], MESH
        ).wait_recv()
    n_l = jnp.zeros((2, TOK), f32)
    a_l = jnp.zeros((2, TOK), f32)
    m_l = jnp.full((2, TOK), very_low, f32)
    a_list, m_list, f_list, l_list = [], [], [], []
    for i in range(NG):
        small_l[i, 0:2, :] = n_l
        small_l[i, 2:4, :] = a_l
        small_l[i, 4:6, :] = m_l
        a_list.append(a_l)
        m_list.append(m_l)
        n_i, a_i, m_i = small1[i, 0:2, :], small1[i, 2:4, :], small1[i, 4:6, :]
        new = jnp.maximum(a_i + m_l, m_i)
        former, latter = jnp.exp(a_i + m_l - new), jnp.exp(m_i - new)
        f_list.append(former)
        l_list.append(latter)
        n_l = former * n_l + latter * n_i
        a_l = a_l + a_i
        m_l = new
    small_t[...] = jnp.zeros_like(small_t)
    small_t[0:2, :] = n_l
    small_t[2:4, :] = a_l
    small_t[4:6, :] = m_l
    for r in range(1, NZ):
        c = copy_to(small_t, small2.at[z], ss.at[2, r], rs.at[2, r], zdev[r])
        c.start()
        pending.append(c)
    small2[z] = small_t[...]

    def mine(pair):
        return jnp.where(g < 4, pair[0:1, :], pair[1:2, :])

    def spread(line):
        return jnp.concatenate([line, line], axis=1)

    for r in range(1, NG):
        copy_to(s_loc.at[0], r1.at[gfrom[r]], ss.at[1, r], rs.at[1, r], gdev[r]).wait_recv()
    run = jnp.zeros((32, DV), f32)
    for i in range(NG):
        pre_l[i] = run
        run = spread(mine(f_list[i])) * run + spread(mine(l_list[i])) * r1[i].astype(f32)
    t_loc[...] = run.astype(bf16)
    for r in range(1, NZ):
        c = copy_to(t_loc, r2.at[z], ss.at[3, r], rs.at[3, r], zdev[r])
        c.start()
        pending.append(c)
    r2[z] = t_loc[...]

    for r in range(1, NZ):
        copy_to(
            small_t, small2.at[lax.rem(z + NZ - r, NZ)], ss.at[2, r], rs.at[2, r], zdev[r]
        ).wait_recv()
    n_z = jnp.zeros((2, TOK), f32)
    m_z = jnp.full((2, TOK), very_low, f32)
    fz, lz = [], []
    for i in range(NZ):
        on = i < z
        n_i, a_i, m_i = small2[i, 0:2, :], small2[i, 2:4, :], small2[i, 4:6, :]
        new = jnp.maximum(a_i + m_z, m_i)
        former, latter = jnp.exp(a_i + m_z - new), jnp.exp(m_i - new)
        former = jnp.where(on, former, 1.0)
        latter = jnp.where(on, latter, 0.0)
        fz.append(mine(former))
        lz.append(mine(latter))
        n_z = former * n_z + latter * n_i
        m_z = jnp.where(on, new, m_z)
    ca, cb = [], []
    for j in range(NG):
        new = jnp.maximum(a_list[j] + m_z, m_list[j])
        ca.append(mine(jnp.exp(m_list[j] - new)))
        cb.append(mine(jnp.exp(a_list[j] + m_z - new)))
    n_g, a_g, m_g = small_l[g, 0:2, :], small_l[g, 2:4, :], small_l[g, 4:6, :]
    m_in = jnp.maximum(a_g + m_z, m_g)
    n_in = jnp.exp(m_g - m_in) * n_g + jnp.exp(a_g + m_z - m_in) * n_z

    scale0, carried, denom = [], [], []
    for h in range(2):
        q_h = q_ref[:, h * DQK : (h + 1) * DQK].astype(f32)
        log_carry = cs_cols[h] + m_in[h : h + 1, 0:1]
        peak = jnp.maximum(peak0[h], log_carry)
        s0, c0 = jnp.exp(peak0[h] - peak), jnp.exp(log_carry - peak) * scale
        normer = s0 * den0[h] + c0 * jnp.sum(q_h * n_in[h : h + 1, :], axis=1, keepdims=True)
        inv = 1.0 / jnp.maximum(jnp.abs(normer), jnp.exp(-peak))
        scale0.append(s0 * inv)
        carried.append(c0 * inv)

    for r in range(1, NZ):
        copy_to(
            t_loc, r2.at[lax.rem(z + NZ - r, NZ)], ss.at[3, r], rs.at[3, r], zdev[r]
        ).wait_recv()
    run = jnp.zeros((32, DV), f32)
    for i in range(NZ):
        run = spread(fz[i]) * run + spread(lz[i]) * r2[i].astype(f32)
    for j in range(NG):
        o3[j] = (spread(ca[j]) * pre_l[j] + spread(cb[j]) * run).astype(bf16)
    for r in range(1, NG):
        c = copy_to(o3.at[gpeer[r]], r3.at[g], ss.at[4, r], rs.at[4, r], gdev[r])
        c.start()
        pending.append(c)
    r3[g] = o3[g]
    gates = [
        hg_ref[:, h * DV : (h + 1) * DV]
        / (1.0 + jnp.exp(-og_ref[:, h * DV : (h + 1) * DV].astype(f32)))
        for h in range(2)
    ]
    for r in range(1, NG):
        copy_to(o3.at[0], r3.at[gfrom[r]], ss.at[4, r], rs.at[4, r], gdev[r]).wait_recv()
    gated, sq = [], jnp.zeros((TOK, 1), f32)
    for h in range(2):
        q_h = q_ref[:, h * DQK : (h + 1) * DQK]
        state = r3[4 * h : 4 * h + 4].reshape(DQK, DV)
        out = scale0[h] * num0[h] + carried[h] * dot(q_h, state)
        sq = sq + jnp.sum(out * out, axis=1, keepdims=True)
        gated.append((out * gates[h]).astype(bf16))
    sq_me[0] = jnp.broadcast_to(row_of(sq, eye), (8, TOK))
    for r in range(1, NX):
        c = copy_to(sq_me.at[0], rsq.at[0, tp], ss.at[5, r], rs.at[5, r], xdev[r])
        c.start()
        pending.append(c)
    rsq[0, tp] = sq_me[0]
    heads = jnp.concatenate(gated, axis=1)
    for r in (2, 1, 3, 0):
        at = pl.multiple_of(xpeer[r] * COLS, COLS)
        part[xpeer[r]] = dot(heads, wo_ref[:, pl.ds(at, COLS)]).astype(bf16)
        if r:
            c = copy_to(part.at[xpeer[r]], rpart.at[tp], ss.at[6, r], rs.at[6, r], xdev[r])
            c.start()
            pending.append(c)
    rpart[tp] = part[tp]
    for r in range(1, NX):
        copy_to(sq_me.at[0], rsq.at[0, xfrom[r]], ss.at[5, r], rs.at[5, r], xdev[r]).wait_recv()
    sq_all = jnp.sum(rsq[0, :, 0, :], axis=0, keepdims=True)
    row_scale = col_of(lax.rsqrt(sq_all / VALS + norm_eps), eye)
    for r in range(1, NX):
        copy_to(part.at[0], rpart.at[xfrom[r]], ss.at[6, r], rs.at[6, r], xdev[r]).wait_recv()
    mixer = rpart[0].astype(f32)
    for i in range(1, NX):
        mixer = mixer + rpart[i].astype(f32)
    resid = (st_ref[...].astype(f32) + mixer * row_scale).astype(bf16)
    resid_ref[...] = resid
    resid_f = resid.astype(f32)
    gain = gain_ref[:, pl.ds(pl.multiple_of(tp * COLS, COLS), COLS)]
    yloc[...] = (resid_f * gain).astype(bf16)
    sq_me[1] = jnp.broadcast_to(
        row_of(jnp.sum(resid_f * resid_f, axis=1, keepdims=True), eye), (8, TOK)
    )
    for r in (2, 1, 3):
        c = copy_to(yloc, y_ref.at[tp], ss.at[8, r], rs.at[8, r], xdev[r])
        c.start()
        pending.append(c)
    for r in range(1, NX):
        c = copy_to(sq_me.at[1], rsq.at[1, tp], ss.at[7, r], rs.at[7, r], xdev[r])
        c.start()
        pending.append(c)
    rsq[1, tp] = sq_me[1]
    y_ref[tp] = yloc[...]
    for r in range(1, NX):
        copy_to(sq_me.at[1], rsq.at[1, xfrom[r]], ss.at[7, r], rs.at[7, r], xdev[r]).wait_recv()
    sq_all = jnp.sum(rsq[1, :, 0, :], axis=0, keepdims=True)
    r_ref[...] = jnp.broadcast_to(
        col_of(lax.rsqrt(sq_all / D + norm_eps), eye), (TOK, TOK)
    )
    for r in range(1, NX):
        copy_to(yloc, y_ref.at[xfrom[r]], ss.at[8, r], rs.at[8, r], xdev[r]).wait_recv()
    for c in pending:
        c.wait_send()


def ffn_kernel(y_ref, r_ref, resid_ref, w_hbm, o_ref, w, acc, part, rpart, lsem, ss, rs):
    sp, tp = lax.axis_index("sp"), lax.axis_index("tp")
    xpeer = [lax.rem(tp + r, NX) for r in range(NX)]
    xfrom = [lax.rem(tp + NX - r, NX) for r in range(NX)]
    xdev = [{"sp": sp, "tp": p} for p in xpeer]
    loads = []
    for i in range(NX):
        loads.append(
            pltpu.make_async_copy(
                w_hbm.at[pl.ds(i * COLS, COLS), pl.ds(0, 2 * FFT)],
                w.at[pl.ds(i * COLS, COLS), pl.ds(0, 2 * FFT)],
                lsem.at[i],
            )
        )
    for i in range(NX):
        loads.append(
            pltpu.make_async_copy(
                w_hbm.at[pl.ds(i * COLS, COLS), pl.ds(2 * FFT, FFT)],
                w.at[pl.ds(i * COLS, COLS), pl.ds(2 * FFT, FFT)],
                lsem.at[NX + i],
            )
        )
    for c in loads:
        c.start()
    bar, count = barrier_all(xdev[1:])
    pl.semaphore_wait(bar, count)
    for i in range(NX):
        loads[i].wait()
        term = dot(y_ref[i], w[i * COLS : (i + 1) * COLS, 0 : 2 * FFT])
        if i == 0:
            acc[...] = term
        else:
            acc[...] += term
    scale = r_ref[:, 0:1]
    gate = acc[:, 0:FFT] * scale
    hidden = (gate / (1.0 + jnp.exp(-gate)) * (acc[:, FFT:] * scale)).astype(bf16)
    for i in range(NX):
        loads[NX + i].wait()
    pending = []
    for r in (2, 1, 3, 0):
        at = pl.multiple_of(xpeer[r] * COLS, COLS)
        part[xpeer[r]] = dot(
            hidden, w[pl.ds(at, COLS), 2 * FFT : 3 * FFT], ((1,), (1,))
        ).astype(bf16)
        if r:
            c = copy_to(part.at[xpeer[r]], rpart.at[tp], ss.at[r], rs.at[r], xdev[r])
            c.start()
            pending.append(c)
    total = resid_ref[...].astype(f32) + part[tp].astype(f32)
    for r in (1, 3, 2):
        copy_to(part.at[0], rpart.at[xfrom[r]], ss.at[r], rs.at[r], xdev[r]).wait_recv()
        total = total + rpart[xfrom[r]].astype(f32)
    o_ref[...] = total.astype(bf16)
    for c in pending:
        c.wait_send()


def local(
    stream,
    queries,
    keys,
    values,
    out_gate,
    input_gate,
    forget_gate,
    head_gain,
    w_out,
    ffn_gain,
    w_gate,
    w_up,
    w_down,
):
    vmem = pl.BlockSpec(memory_space=pltpu.VMEM)
    both = jnp.concatenate([w_gate, w_up, w_down.T], axis=1)
    weights = lax.all_gather(both, "sp", axis=0, tiled=True)
    y, r, resid = pl.pallas_call(
        cell_kernel,
        out_shape=(
            jax.ShapeDtypeStruct((NX, TOK, COLS), bf16),
            jax.ShapeDtypeStruct((TOK, TOK), f32),
            jax.ShapeDtypeStruct((TOK, COLS), bf16),
        ),
        in_specs=[vmem] * 10,
        out_specs=(vmem, vmem, vmem),
        scratch_shapes=[
            pltpu.VMEM((NG, 8, TOK), f32),
            pltpu.VMEM((NZ, 8, TOK), f32),
            pltpu.VMEM((NG, 8, TOK), f32),
            pltpu.VMEM((8, TOK), f32),
            pltpu.VMEM((8, TOK), f32),
            pltpu.VMEM((NG, 32, DV), bf16),
            pltpu.VMEM((NG, 32, DV), bf16),
            pltpu.VMEM((NG, 32, DV), f32),
            pltpu.VMEM((32, DV), bf16),
            pltpu.VMEM((NZ, 32, DV), bf16),
            pltpu.VMEM((NG, 32, DV), bf16),
            pltpu.VMEM((NG, 32, DV), bf16),
            pltpu.VMEM((NX, TOK, COLS), bf16),
            pltpu.VMEM((NX, TOK, COLS), bf16),
            pltpu.VMEM((2, 8, TOK), f32),
            pltpu.VMEM((2, NX, 8, TOK), f32),
            pltpu.VMEM((TOK, COLS), bf16),
            pltpu.SemaphoreType.DMA((9, 8)),
            pltpu.SemaphoreType.DMA((9, 8)),
        ],
        compiler_params=pltpu.CompilerParams(collective_id=0, has_side_effects=True),
        cost_estimate=pl.CostEstimate(flops=50_000_000_000, bytes_accessed=4_000_000, transcendentals=0),
    )(
        queries,
        keys,
        values,
        out_gate,
        input_gate,
        forget_gate,
        head_gain.reshape(1, COLS),
        w_out,
        stream,
        ffn_gain.reshape(1, D),
    )
    return pl.pallas_call(
        ffn_kernel,
        out_shape=jax.ShapeDtypeStruct((TOK, COLS), bf16),
        in_specs=[vmem, vmem, vmem, pl.BlockSpec(memory_space=pl.ANY)],
        out_specs=vmem,
        scratch_shapes=[
            pltpu.VMEM((D, 3 * FFT), bf16),
            pltpu.VMEM((TOK, 2 * FFT), f32),
            pltpu.VMEM((NX, TOK, COLS), bf16),
            pltpu.VMEM((NX, TOK, COLS), bf16),
            pltpu.SemaphoreType.DMA((8,)),
            pltpu.SemaphoreType.DMA((NX,)),
            pltpu.SemaphoreType.DMA((NX,)),
        ],
        compiler_params=pltpu.CompilerParams(collective_id=1, has_side_effects=True, vmem_limit_bytes=56 * 2**20),
    )(y, r, resid, weights)


def solution(mesh):
    in_specs = (
        P("sp", "tp"),
        P("sp", "tp"),
        P("sp", "tp"),
        P("sp", "tp"),
        P("sp", "tp"),
        P("sp", "tp"),
        P("sp", "tp"),
        P("tp"),
        P("tp", None),
        P(),
        P("sp", "tp"),
        P("sp", "tp"),
        P("tp", "sp"),
    )
    return jax.shard_map(
        local, mesh=mesh, in_specs=in_specs, out_specs=P("sp", "tp"), check_vma=False
    )
```

```python
import functools

import jax
import jax.numpy as jnp
from jax import lax
from jax.experimental import pallas as pl
from jax.experimental.pallas import tpu as pltpu
from jax.sharding import PartitionSpec as P

D = 2048
DQK = 128
DV = 256
VALS = 2048
FFT = 1408
TOK = 128
COLS = 512
NG = 8
NZ = 8
NX = 4
norm_eps = 1e-06
very_low = -1e30
MESH = pl.DeviceIdType.MESH
f32 = jnp.float32
bf16 = jnp.bfloat16


def row_of(col, eye):
    return jnp.sum(jnp.where(eye, col, 0.0), axis=0, keepdims=True)


def col_of(row, eye):
    return jnp.sum(jnp.where(eye, row, 0.0), axis=1, keepdims=True)


def split_hi_lo(x):
    hi = x.astype(bf16)
    return hi, (x - hi.astype(f32)).astype(bf16)


def dot(a, b, dims=((1,), (0,))):
    return lax.dot_general(a, b, (dims, ((), ())), preferred_element_type=f32)


def log_sigmoid(x):
    return jnp.minimum(x, 0.0) - jnp.log1p(jnp.exp(-jnp.abs(x)))


def copy_to(src, dst, ssem, rsem, dev):
    return pltpu.make_async_remote_copy(
        src_ref=src, dst_ref=dst, send_sem=ssem, recv_sem=rsem, device_id=dev, device_id_type=MESH
    )


def barrier_all(devs):
    bar = pltpu.get_barrier_semaphore()
    for dev in devs:
        pl.semaphore_signal(bar, inc=1, device_id=dev, device_id_type=MESH)
    return bar, len(devs)


class Weights:
    def __init__(self, w, wss, wrs, z, g, tp):
        self.w, self.wss, self.wrs = w, wss, wrs
        self.z, self.y, self.c, self.tp = z, g // 2, lax.rem(g, 2), tp
        self.ids, self.sent = {}, []
        self.zi = [lax.rem(z + k, NZ) for k in (0, 7, 1, 6, 2, 5, 3, 4)]
        z_at = lambda k: {"sp": lax.rem(z + k, NZ) * NG + g, "tp": tp}
        y_at = lambda k: {"sp": z * NG + lax.rem(self.y + k, 4) * 2 + self.c, "tp": tp}
        self.dev = {
            "z+": z_at(1),
            "z-": z_at(7),
            "y+": y_at(1),
            "y-": y_at(3),
            "s": {"sp": z * NG + self.y * 2 + (1 - self.c), "tp": tp},
        }

    def zk(self, k):
        return lax.rem(self.z + NZ + k, NZ)

    def yk(self, k):
        return lax.rem(self.y + 4 + k, 4)

    def both(self, zi, yi):
        return (pl.ds(0, 2), zi, yi, self.c)

    def desc(self, name, way, at):
        n = self.ids.setdefault((name, way), len(self.ids))
        return copy_to(self.w.at[at], self.w.at[at], self.wss.at[n], self.wrs.at[n], self.dev[way])

    def send(self, name, way, at):
        c = self.desc(name, way, at)
        c.start()
        self.sent.append(c)

    def got(self, name, way, at):
        self.desc(name, way, at).wait_recv()

    def first(self):
        own = self.both(self.z, self.y)
        self.send("bz1", "z+", own)
        self.send("bz1", "z-", own)
        down = (2, self.z, self.y, self.c)
        self.send("ay", "y+", down)
        self.send("ay", "y-", down)
        self.by(0)

    def bz(self, k):
        back, ahead = self.zk(-k), self.zk(k)
        if k == 4:
            self.got("bz4", "z+", (0, back, self.y, self.c))
            self.got("bz4", "z-", (1, ahead, self.y, self.c))
            return
        self.got(f"bz{k}", "z+", self.both(back, self.y))
        self.got(f"bz{k}", "z-", self.both(ahead, self.y))
        if k == 3:
            self.send("bz4", "z+", (0, back, self.y, self.c))
            self.send("bz4", "z-", (1, ahead, self.y, self.c))
        else:
            self.send(f"bz{k + 1}", "z+", self.both(back, self.y))
            self.send(f"bz{k + 1}", "z-", self.both(ahead, self.y))

    def by(self, j):
        self.send(f"by{j}", "y+", self.both(self.zi[j], self.y))
        self.send(f"by{j}", "y-", self.both(self.zi[j], self.y))

    def byf(self, j):
        self.got(f"by{j}", "y+", self.both(self.zi[j], self.yk(-1)))
        self.send(f"byf{j}", "y+", (0, self.zi[j], self.yk(-1), self.c))
        self.got(f"by{j}", "y-", self.both(self.zi[j], self.yk(1)))
        self.send(f"byf{j}", "y-", (1, self.zi[j], self.yk(1), self.c))

    def sb(self, j):
        self.got(f"byf{j}", "y+", (0, self.zi[j], self.yk(-2), self.c))
        self.got(f"byf{j}", "y-", (1, self.zi[j], self.yk(2), self.c))
        self.send(f"sb{j}", "s", (pl.ds(0, 2), self.zi[j], pl.ds(0, 4), self.c))

    def ayf(self):
        self.got("ay", "y+", (2, self.z, self.yk(-1), self.c))
        self.send("ayf", "y+", (2, self.z, self.yk(-1), self.c, pl.ds(0, 16)))
        self.got("ay", "y-", (2, self.z, self.yk(1), self.c))
        self.send("ayf", "y-", (2, self.z, self.yk(1), self.c, pl.ds(16, 16)))

    def pair(self, zi, p):
        return (2, zi, pl.ds(2 * p, 2), self.c)

    def sa(self, k):
        self.send(f"sa{k}", "s", (2, self.zk(k), pl.ds(0, 4), self.c))

    def az(self, k):
        if k == 0:
            self.got("ayf", "y+", (2, self.z, self.yk(-2), self.c, pl.ds(0, 16)))
            self.got("ayf", "y-", (2, self.z, self.yk(2), self.c, pl.ds(16, 16)))
        back, ahead = self.zk(-k), self.zk(k)
        if k == 4:
            self.got("az4", "z+", self.pair(back, 0))
            self.got("az4", "z-", self.pair(ahead, 1))
            self.sa(4)
            return
        for p in range(2):
            if k:
                self.got(f"az{k}{p}", "z+", self.pair(back, p))
            if k < 3:
                self.send(f"az{k + 1}{p}", "z+", self.pair(back, p))
            elif p == 0:
                self.send("az4", "z+", self.pair(back, 0))
            if k:
                self.got(f"az{k}{p}", "z-", self.pair(ahead, p))
            if k < 3:
                self.send(f"az{k + 1}{p}", "z-", self.pair(ahead, p))
            elif p == 1:
                self.send("az4", "z-", self.pair(ahead, 1))
        self.sa(-k)
        if k:
            self.sa(k)

    def after_slices(self):
        self.bz(1)
        self.ayf()
        self.byf(0)
        self.by(1)
        self.by(2)

    def after_totals(self):
        self.bz(2)
        self.az(0)

    def after_prefixes(self):
        self.bz(3)
        for j in (3, 4, 5, 6):
            self.by(j)
        self.byf(1)
        self.byf(2)

    def after_partials(self):
        self.bz(4)
        self.by(7)
        self.az(1)
        self.sb(0)

    def after_features(self):
        self.az(2)
        for j in (1, 2):
            self.sb(j)
        for j in (3, 4):
            self.byf(j)

    def before_column(self, j):
        if j == 0:
            self.az(3)
            for k in (5, 6, 7):
                self.byf(k)
        if j >= 3:
            self.sb(j)
        if j == 5:
            self.az(4)
        self.got(f"sb{j}", "s", (pl.ds(0, 2), self.zi[j], pl.ds(0, 4), 1 - self.c))

    def before_down(self):
        for k in (0, -1, 1, -2, 2, -3, 3, 4):
            self.got(f"sa{k}", "s", (2, self.zk(k), pl.ds(0, 4), 1 - self.c))


def layer_kernel(
    q_ref,
    k_ref,
    v_ref,
    og_ref,
    ig_ref,
    fg_ref,
    hg_ref,
    wo_hbm,
    st_ref,
    gain_ref,
    wg_hbm,
    wu_hbm,
    wd_hbm,
    o_ref,
    w,
    wo,
    acc,
    y_ref,
    small1,
    small2,
    small_l,
    small_me,
    small_t,
    s_loc,
    r1,
    pre_l,
    t_loc,
    r2,
    o3,
    r3,
    part,
    rpart,
    sq_me,
    rsq,
    yloc,
    part2,
    rpart2,
    lsem,
    ss,
    rs,
    wss,
    wrs,
):
    sp, tp = lax.axis_index("sp"), lax.axis_index("tp")
    z, g = sp // NG, lax.rem(sp, NG)
    gpeer = [lax.rem(g + r, NG) for r in range(NG)]
    gfrom = [lax.rem(g + NG - r, NG) for r in range(NG)]
    zpeer = [lax.rem(z + r, NZ) for r in range(NZ)]
    xpeer = [lax.rem(tp + r, NX) for r in range(NX)]
    xfrom = [lax.rem(tp + NX - r, NX) for r in range(NX)]
    gdev = [{"sp": z * NG + p, "tp": tp} for p in gpeer]
    zdev = [{"sp": p * NG + g, "tp": tp} for p in zpeer]
    xdev = [{"sp": sp, "tp": p} for p in xpeer]
    bar, count = barrier_all(gdev[1:] + zdev[1:] + xdev[1:])
    net = Weights(w, wss, wrs, z, g, tp)
    loads = [
        pltpu.make_async_copy(ref, w.at[kind, z, net.y, net.c], lsem.at[kind])
        for kind, ref in enumerate((wg_hbm, wu_hbm, wd_hbm))
    ]
    loads.append(pltpu.make_async_copy(wo_hbm, wo, lsem.at[3]))
    for c in loads:
        c.start()

    rows = lax.broadcasted_iota(jnp.int32, (TOK, TOK), 0)
    cols = lax.broadcasted_iota(jnp.int32, (TOK, TOK), 1)
    eye = rows == cols
    low = rows >= cols

    lf = log_sigmoid(fg_ref[...])
    ig = ig_ref[...]
    small_me[...] = jnp.zeros_like(small_me)
    cs_cols, pairs, wks = [], [], []
    for h in range(2):
        lf_row = lf[h : h + 1, :]
        lf_col = col_of(lf_row, eye)
        cs_col = jnp.sum(jnp.where(low, lf_row, 0.0), axis=1, keepdims=True)
        cs_row = jnp.sum(jnp.where(rows <= cols, lf_col, 0.0), axis=0, keepdims=True)
        ig_row = ig[h : h + 1, :]
        rest_row = ig_row - cs_row
        rest_col = col_of(rest_row, eye)
        top = jnp.max(rest_row, axis=1, keepdims=True)
        total = jnp.sum(lf_row, axis=1, keepdims=True)
        wk = jnp.exp(rest_col - top) * k_ref[:, h * DQK : (h + 1) * DQK].astype(f32)
        small_me[h : h + 1, :] = jnp.sum(wk, axis=0, keepdims=True)
        small_me[2 + h : 3 + h, :] = jnp.broadcast_to(total, (1, TOK))
        small_me[4 + h : 5 + h, :] = jnp.broadcast_to(total + top, (1, TOK))
        cs_cols.append(cs_col)
        pairs.append((rest_row, ig_row))
        wks.append(wk)
    pl.semaphore_wait(bar, count)
    pending = []
    for r in range(1, NG):
        c = copy_to(small_me, small1.at[g], ss.at[0, r], rs.at[0, r], gdev[r])
        c.start()
        pending.append(c)
    small1[g] = small_me[...]
    for c in loads[:3]:
        c.wait()
    net.first()

    for h in range(2):
        hi, lo = split_hi_lo(wks[h])
        v_h = v_ref[:, h * DV : (h + 1) * DV]
        state = dot(hi, v_h, ((0,), (0,))) + dot(lo, v_h, ((0,), (0,)))
        s_loc[4 * h : 4 * h + 4] = state.astype(bf16).reshape(4, 32, DV)
    for r in range(1, NG):
        c = copy_to(s_loc.at[gpeer[r]], r1.at[g], ss.at[1, r], rs.at[1, r], gdev[r])
        c.start()
        pending.append(c)
    r1[g] = s_loc[g]
    net.after_slices()

    scale = DQK**-0.5
    num0, den0, peak0 = [], [], []
    for h in range(2):
        rest_row, ig_row = pairs[h]
        q_h = q_ref[:, h * DQK : (h + 1) * DQK]
        k_h = k_ref[:, h * DQK : (h + 1) * DQK]
        log_pair = jnp.where(low, cs_cols[h] + rest_row, -jnp.inf)
        peak = jnp.max(log_pair, axis=1, keepdims=True)
        scores = dot(q_h, k_h, ((1,), (1,))) * scale * jnp.exp(log_pair - peak)
        hi, lo = split_hi_lo(scores)
        v_h = v_ref[:, h * DV : (h + 1) * DV]
        num0.append(dot(hi, v_h) + dot(lo, v_h))
        den0.append(jnp.sum(scores, axis=1, keepdims=True))
        peak0.append(peak)

    for r in range(1, NG):
        pltpu.make_async_remote_copy(
            small_me, small1.at[gfrom[r]], ss.at[0, r], rs.at[0, r], gdev[r], MESH
        ).wait_recv()
    n_l = jnp.zeros((2, TOK), f32)
    a_l = jnp.zeros((2, TOK), f32)
    m_l = jnp.full((2, TOK), very_low, f32)
    a_list, m_list, f_list, l_list = [], [], [], []
    for i in range(NG):
        small_l[i, 0:2, :] = n_l
        small_l[i, 2:4, :] = a_l
        small_l[i, 4:6, :] = m_l
        a_list.append(a_l)
        m_list.append(m_l)
        n_i, a_i, m_i = small1[i, 0:2, :], small1[i, 2:4, :], small1[i, 4:6, :]
        new = jnp.maximum(a_i + m_l, m_i)
        former, latter = jnp.exp(a_i + m_l - new), jnp.exp(m_i - new)
        f_list.append(former)
        l_list.append(latter)
        n_l = former * n_l + latter * n_i
        a_l = a_l + a_i
        m_l = new
    small_t[...] = jnp.zeros_like(small_t)
    small_t[0:2, :] = n_l
    small_t[2:4, :] = a_l
    small_t[4:6, :] = m_l
    for r in range(1, NZ):
        c = copy_to(small_t, small2.at[z], ss.at[2, r], rs.at[2, r], zdev[r])
        c.start()
        pending.append(c)
    small2[z] = small_t[...]

    def mine(pair):
        return jnp.where(g < 4, pair[0:1, :], pair[1:2, :])

    def spread(line):
        return jnp.concatenate([line, line], axis=1)

    for r in range(1, NG):
        copy_to(s_loc.at[0], r1.at[gfrom[r]], ss.at[1, r], rs.at[1, r], gdev[r]).wait_recv()
    run = jnp.zeros((32, DV), f32)
    for i in range(NG):
        pre_l[i] = run
        run = spread(mine(f_list[i])) * run + spread(mine(l_list[i])) * r1[i].astype(f32)
    t_loc[...] = run.astype(bf16)
    for r in range(1, NZ):
        c = copy_to(t_loc, r2.at[z], ss.at[3, r], rs.at[3, r], zdev[r])
        c.start()
        pending.append(c)
    r2[z] = t_loc[...]
    net.after_totals()

    for r in range(1, NZ):
        copy_to(
            small_t, small2.at[lax.rem(z + NZ - r, NZ)], ss.at[2, r], rs.at[2, r], zdev[r]
        ).wait_recv()
    n_z = jnp.zeros((2, TOK), f32)
    m_z = jnp.full((2, TOK), very_low, f32)
    fz, lz = [], []
    for i in range(NZ):
        on = i < z
        n_i, a_i, m_i = small2[i, 0:2, :], small2[i, 2:4, :], small2[i, 4:6, :]
        new = jnp.maximum(a_i + m_z, m_i)
        former, latter = jnp.exp(a_i + m_z - new), jnp.exp(m_i - new)
        former = jnp.where(on, former, 1.0)
        latter = jnp.where(on, latter, 0.0)
        fz.append(mine(former))
        lz.append(mine(latter))
        n_z = former * n_z + latter * n_i
        m_z = jnp.where(on, new, m_z)
    ca, cb = [], []
    for j in range(NG):
        new = jnp.maximum(a_list[j] + m_z, m_list[j])
        ca.append(mine(jnp.exp(m_list[j] - new)))
        cb.append(mine(jnp.exp(a_list[j] + m_z - new)))
    n_g, a_g, m_g = small_l[g, 0:2, :], small_l[g, 2:4, :], small_l[g, 4:6, :]
    m_in = jnp.maximum(a_g + m_z, m_g)
    n_in = jnp.exp(m_g - m_in) * n_g + jnp.exp(a_g + m_z - m_in) * n_z

    scale0, carried, denom = [], [], []
    for h in range(2):
        q_h = q_ref[:, h * DQK : (h + 1) * DQK].astype(f32)
        log_carry = cs_cols[h] + m_in[h : h + 1, 0:1]
        peak = jnp.maximum(peak0[h], log_carry)
        s0, c0 = jnp.exp(peak0[h] - peak), jnp.exp(log_carry - peak) * scale
        normer = s0 * den0[h] + c0 * jnp.sum(q_h * n_in[h : h + 1, :], axis=1, keepdims=True)
        inv = 1.0 / jnp.maximum(jnp.abs(normer), jnp.exp(-peak))
        scale0.append(s0 * inv)
        carried.append(c0 * inv)

    for r in range(1, NZ):
        copy_to(
            t_loc, r2.at[lax.rem(z + NZ - r, NZ)], ss.at[3, r], rs.at[3, r], zdev[r]
        ).wait_recv()
    run = jnp.zeros((32, DV), f32)
    for i in range(NZ):
        run = spread(fz[i]) * run + spread(lz[i]) * r2[i].astype(f32)
    for j in range(NG):
        o3[j] = (spread(ca[j]) * pre_l[j] + spread(cb[j]) * run).astype(bf16)
    for r in range(1, NG):
        c = copy_to(o3.at[gpeer[r]], r3.at[g], ss.at[4, r], rs.at[4, r], gdev[r])
        c.start()
        pending.append(c)
    r3[g] = o3[g]
    net.after_prefixes()
    gates = [
        hg_ref[:, h * DV : (h + 1) * DV]
        / (1.0 + jnp.exp(-og_ref[:, h * DV : (h + 1) * DV].astype(f32)))
        for h in range(2)
    ]
    for r in range(1, NG):
        copy_to(o3.at[0], r3.at[gfrom[r]], ss.at[4, r], rs.at[4, r], gdev[r]).wait_recv()
    gated, sq = [], jnp.zeros((TOK, 1), f32)
    for h in range(2):
        q_h = q_ref[:, h * DQK : (h + 1) * DQK]
        state = r3[4 * h : 4 * h + 4].reshape(DQK, DV)
        out = scale0[h] * num0[h] + carried[h] * dot(q_h, state)
        sq = sq + jnp.sum(out * out, axis=1, keepdims=True)
        gated.append((out * gates[h]).astype(bf16))
    sq_me[0] = jnp.broadcast_to(row_of(sq, eye), (8, TOK))
    for r in range(1, NX):
        c = copy_to(sq_me.at[0], rsq.at[0, tp], ss.at[5, r], rs.at[5, r], xdev[r])
        c.start()
        pending.append(c)
    rsq[0, tp] = sq_me[0]
    heads = jnp.concatenate(gated, axis=1)
    loads[3].wait()
    for r in (2, 1, 3, 0):
        at = pl.multiple_of(xpeer[r] * COLS, COLS)
        part[xpeer[r]] = dot(heads, wo[:, pl.ds(at, COLS)]).astype(bf16)
        if r:
            c = copy_to(part.at[xpeer[r]], rpart.at[tp], ss.at[6, r], rs.at[6, r], xdev[r])
            c.start()
            pending.append(c)
    rpart[tp] = part[tp]
    net.after_partials()
    for r in range(1, NX):
        copy_to(sq_me.at[0], rsq.at[0, xfrom[r]], ss.at[5, r], rs.at[5, r], xdev[r]).wait_recv()
    sq_all = jnp.sum(rsq[0, :, 0, :], axis=0, keepdims=True)
    row_scale = col_of(lax.rsqrt(sq_all / VALS + norm_eps), eye)
    for r in range(1, NX):
        copy_to(part.at[0], rpart.at[xfrom[r]], ss.at[6, r], rs.at[6, r], xdev[r]).wait_recv()
    mixer = rpart[0].astype(f32)
    for i in range(1, NX):
        mixer = mixer + rpart[i].astype(f32)
    resid = (st_ref[...].astype(f32) + mixer * row_scale).astype(bf16)
    resid_f = resid.astype(f32)
    gain = gain_ref[:, pl.ds(pl.multiple_of(tp * COLS, COLS), COLS)]
    yloc[...] = (resid_f * gain).astype(bf16)
    sq_me[1] = jnp.broadcast_to(
        row_of(jnp.sum(resid_f * resid_f, axis=1, keepdims=True), eye), (8, TOK)
    )
    for r in (2, 1, 3):
        c = copy_to(yloc, y_ref.at[tp], ss.at[8, r], rs.at[8, r], xdev[r])
        c.start()
        pending.append(c)
    for r in range(1, NX):
        c = copy_to(sq_me.at[1], rsq.at[1, tp], ss.at[7, r], rs.at[7, r], xdev[r])
        c.start()
        pending.append(c)
    rsq[1, tp] = sq_me[1]
    y_ref[tp] = yloc[...]
    net.after_features()
    for r in range(1, NX):
        copy_to(sq_me.at[1], rsq.at[1, xfrom[r]], ss.at[7, r], rs.at[7, r], xdev[r]).wait_recv()
    sq_all = jnp.sum(rsq[1, :, 0, :], axis=0, keepdims=True)
    scale_in = col_of(lax.rsqrt(sq_all / D + norm_eps), eye)
    for r in range(1, NX):
        copy_to(yloc, y_ref.at[xfrom[r]], ss.at[8, r], rs.at[8, r], xdev[r]).wait_recv()
    for j in range(NZ):
        net.before_column(j)
        zi = net.zi[j]
        y_col = y_ref[zi // 2, :, pl.ds(pl.multiple_of(lax.rem(zi, 2) * 256, 256), 256)]
        for kind in range(2):
            term = dot(y_col, w[kind, zi].reshape(256, FFT))
            if j == 0:
                acc[kind] = term
            else:
                acc[kind] += term
    gate = acc[0] * scale_in
    hidden = (gate / (1.0 + jnp.exp(-gate)) * (acc[1] * scale_in)).astype(bf16)
    net.before_down()
    for r in (2, 1, 3, 0):
        at = xpeer[r]
        part2[at] = dot(
            hidden, w[2, pl.ds(2 * at, 2)].reshape(COLS, FFT), ((1,), (1,))
        ).astype(bf16)
        if r:
            c = copy_to(part2.at[at], rpart2.at[tp], ss.at[9, r], rs.at[9, r], xdev[r])
            c.start()
            pending.append(c)
    total = resid_f + part2[tp].astype(f32)
    for r in (1, 3, 2):
        copy_to(part2.at[0], rpart2.at[xfrom[r]], ss.at[9, r], rs.at[9, r], xdev[r]).wait_recv()
        total = total + rpart2[xfrom[r]].astype(f32)
    o_ref[...] = total.astype(bf16)
    for c in pending + net.sent:
        c.wait_send()


def local(
    stream,
    queries,
    keys,
    values,
    out_gate,
    input_gate,
    forget_gate,
    head_gain,
    w_out,
    ffn_gain,
    w_gate,
    w_up,
    w_down,
):
    vmem = pl.BlockSpec(memory_space=pltpu.VMEM)
    hbm = pl.BlockSpec(memory_space=pl.ANY)
    return pl.pallas_call(
        layer_kernel,
        out_shape=jax.ShapeDtypeStruct((TOK, COLS), bf16),
        in_specs=[vmem] * 7 + [hbm] + [vmem] * 2 + [hbm] * 3,
        out_specs=vmem,
        scratch_shapes=[
            pltpu.VMEM((3, NZ, 4, 2, 32, FFT), bf16),
            pltpu.VMEM((COLS, D), bf16),
            pltpu.VMEM((2, TOK, FFT), f32),
            pltpu.VMEM((NX, TOK, COLS), bf16),
            pltpu.VMEM((NG, 8, TOK), f32),
            pltpu.VMEM((NZ, 8, TOK), f32),
            pltpu.VMEM((NG, 8, TOK), f32),
            pltpu.VMEM((8, TOK), f32),
            pltpu.VMEM((8, TOK), f32),
            pltpu.VMEM((NG, 32, DV), bf16),
            pltpu.VMEM((NG, 32, DV), bf16),
            pltpu.VMEM((NG, 32, DV), f32),
            pltpu.VMEM((32, DV), bf16),
            pltpu.VMEM((NZ, 32, DV), bf16),
            pltpu.VMEM((NG, 32, DV), bf16),
            pltpu.VMEM((NG, 32, DV), bf16),
            pltpu.VMEM((NX, TOK, COLS), bf16),
            pltpu.VMEM((NX, TOK, COLS), bf16),
            pltpu.VMEM((2, 8, TOK), f32),
            pltpu.VMEM((2, NX, 8, TOK), f32),
            pltpu.VMEM((TOK, COLS), bf16),
            pltpu.VMEM((NX, TOK, COLS), bf16),
            pltpu.VMEM((NX, TOK, COLS), bf16),
            pltpu.SemaphoreType.DMA((4,)),
            pltpu.SemaphoreType.DMA((10, 8)),
            pltpu.SemaphoreType.DMA((10, 8)),
            pltpu.SemaphoreType.DMA((96,)),
            pltpu.SemaphoreType.DMA((96,)),
        ],
        compiler_params=pltpu.CompilerParams(
            collective_id=0, has_side_effects=True, vmem_limit_bytes=60 * 2**20
        ),
    )(
        queries,
        keys,
        values,
        out_gate,
        input_gate.T,
        forget_gate.T,
        head_gain.reshape(1, COLS),
        w_out,
        stream,
        ffn_gain.reshape(1, D),
        w_gate,
        w_up,
        w_down.T,
    )


def solution(mesh):
    in_specs = (
        P("sp", "tp"),
        P("sp", "tp"),
        P("sp", "tp"),
        P("sp", "tp"),
        P("sp", "tp"),
        P("sp", "tp"),
        P("sp", "tp"),
        P("tp"),
        P("tp", None),
        P(),
        P("sp", "tp"),
        P("sp", "tp"),
        P("tp", "sp"),
    )
    return jax.shard_map(
        local, mesh=mesh, in_specs=in_specs, out_specs=P("sp", "tp"), check_vma=False
    )
```

```python
import functools

import jax
import jax.numpy as jnp
from jax import lax
from jax.experimental import pallas as pl
from jax.experimental.pallas import tpu as pltpu
from jax.sharding import PartitionSpec as P

D = 2048
DQK = 128
DV = 256
VALS = 2048
FFT = 1408
TOK = 128
COLS = 512
NG = 8
NZ = 8
NX = 4
norm_eps = 1e-06
very_low = -1e30
MESH = pl.DeviceIdType.MESH
f32 = jnp.float32
bf16 = jnp.bfloat16


def row_of(col, eye):
    return jnp.sum(jnp.where(eye, col, 0.0), axis=0, keepdims=True)


def col_of(row, eye):
    return jnp.sum(jnp.where(eye, row, 0.0), axis=1, keepdims=True)


def split_hi_lo(x):
    hi = x.astype(bf16)
    return hi, (x - hi.astype(f32)).astype(bf16)


def dot(a, b, dims=((1,), (0,))):
    return lax.dot_general(a, b, (dims, ((), ())), preferred_element_type=f32)


def log_sigmoid(x):
    return jnp.minimum(x, 0.0) - jnp.log1p(jnp.exp(-jnp.abs(x)))


def copy_to(src, dst, ssem, rsem, dev):
    return pltpu.make_async_remote_copy(
        src_ref=src, dst_ref=dst, send_sem=ssem, recv_sem=rsem, device_id=dev, device_id_type=MESH
    )


def barrier_all(devs):
    bar = pltpu.get_barrier_semaphore()
    for dev in devs:
        pl.semaphore_signal(bar, inc=1, device_id=dev, device_id_type=MESH)
    return bar, len(devs)


COLUMNS = (0, -1, 1, -2, 2, -3, 3, 4)
SPLIT = {"u": 512, "d": 640}
STEPS = {
    "first": (
        ("own", "u"),
        ("by", "u", 0),
    ),
    "slices": (
        ("ayf", "u"),
    ),
    "totals": (
        ("bz", "u", 1),
        ("by", "u", 1),
        ("by", "u", 2),
        ("byf", "u", 0),
        ("az", "u", 0),
        ("own", "d"),
        ("by", "d", 0),
        ("byf", "u", 1),
    ),
    "prefix": (
        ("bz", "u", 2),
        ("by", "u", 3),
        ("by", "u", 4),
        ("byf", "u", 2),
        ("sb", "u", 0),
    ),
    "parts": (
        ("az", "u", 1),
        ("sb", "u", 1),
        ("ayf", "d"),
        ("byf", "d", 0),
        ("bz", "d", 1),
        ("bz", "u", 3),
        ("by", "u", 5),
        ("by", "u", 6),
        ("byf", "u", 3),
        ("byf", "u", 4),
        ("sb", "u", 2),
        ("az", "d", 0),
        ("sb", "d", 0),
    ),
    "feats": (
        ("az", "u", 2),
        ("by", "d", 1),
        ("byf", "u", 5),
        ("bz", "u", 4),
        ("by", "u", 7),
        ("byf", "u", 6),
        ("sb", "u", 3),
        ("bz", "d", 2),
        ("sb", "u", 4),
        ("az", "d", 1),
        ("by", "d", 2),
    ),
    "rest": (
        ("fa", "u", -2),
        ("fa", "u", -1),
        ("fb", "u", 0),
        ("fa", "u", 0),
        ("fb", "u", 1),
        ("fa", "u", 1),
        ("sb", "u", 5),
        ("fb", "u", 2),
        ("fa", "u", 2),
        ("fb", "u", 3),
        ("fb", "u", 4),
        ("by", "d", 3),
        ("by", "d", 4),
        ("byf", "d", 1),
        ("byf", "u", 7),
        ("az", "u", 3),
        ("fb", "u", 5),
        ("sb", "u", 6),
        ("bz", "d", 3),
        ("by", "d", 5),
        ("by", "d", 6),
        ("fa", "u", -3),
        ("byf", "d", 2),
        ("fa", "u", 3),
        ("byf", "d", 3),
        ("fb", "u", 6),
        ("byf", "d", 4),
        ("az", "d", 2),
        ("sb", "d", 1),
        ("sb", "u", 7),
        ("byf", "d", 5),
        ("az", "u", 4),
        ("bz", "d", 4),
        ("by", "d", 7),
        ("byf", "d", 6),
        ("sb", "d", 2),
        ("fb", "u", 7),
        ("sb", "d", 3),
        ("fa", "u", 4),
        ("hid", "u"),
        ("sb", "d", 4),
        ("sb", "d", 5),
        ("dn", "d", 0),
        ("byf", "d", 7),
        ("az", "d", 3),
        ("sb", "d", 6),
        ("dn", "d", 3),
        ("sb", "d", 7),
        ("dn", "d", 1),
        ("az", "d", 4),
        ("dn", "d", 2),
    ),
}


class Weights:
    def __init__(self, w, wss, wrs, z, g, tp):
        self.w, self.wss, self.wrs = w, wss, wrs
        self.z, self.y, self.c, self.tp = z, g // 2, lax.rem(g, 2), tp
        self.ids, self.sent = {}, []
        self.zi = [self.zk(k) for k in COLUMNS]

        def z_at(k):
            return {"sp": lax.rem(z + k, NZ) * NG + g, "tp": tp}

        def y_at(k):
            return {"sp": z * NG + lax.rem(self.y + k, 4) * 2 + self.c, "tp": tp}

        self.dev = {
            "z+": z_at(1),
            "z-": z_at(7),
            "y+": y_at(1),
            "y-": y_at(3),
            "s": {"sp": z * NG + self.y * 2 + (1 - self.c), "tp": tp},
        }

    def zk(self, k):
        return lax.rem(self.z + NZ + k, NZ)

    def yk(self, k):
        return lax.rem(self.y + 4 + k, 4)

    def lanes(self, f, route):
        cut = SPLIT[f]
        return pl.ds(0, cut) if route == "a" else pl.ds(cut, FFT - cut)

    def at(self, f, route, zi, yi, half=None, core=None):
        lanes, rows = self.lanes(f, route), pl.ds(0, 32)
        if f == "u":
            kind = pl.ds(0, 2) if half is None else half
        else:
            kind = 2
            rows = rows if half is None else pl.ds(16 * half, 16)
        return (kind, zi, yi, self.c if core is None else core, rows, lanes)

    def desc(self, name, way, at):
        n = self.ids.setdefault((name, way), len(self.ids))
        return copy_to(self.w.at[at], self.w.at[at], self.wss.at[n], self.wrs.at[n], self.dev[way])

    def send(self, name, way, at):
        c = self.desc(name, way, at)
        c.start()
        self.sent.append(c)

    def got(self, name, way, at):
        self.desc(name, way, at).wait_recv()

    def own(self, f):
        for way in ("z+", "z-"):
            self.send(f"bz{f}1", way, self.at(f, "b", self.z, self.y))
        for way in ("y+", "y-"):
            self.send(f"ay{f}", way, self.at(f, "a", self.z, self.y))

    def bz(self, f, k):
        back, ahead = self.zk(-k), self.zk(k)
        halves = (0, 1) if k == 4 else (None, None)
        self.got(f"bz{f}{k}", "z+", self.at(f, "b", back, self.y, halves[0]))
        self.got(f"bz{f}{k}", "z-", self.at(f, "b", ahead, self.y, halves[1]))
        if k < 4:
            halves = (0, 1) if k == 3 else (None, None)
            self.send(f"bz{f}{k + 1}", "z+", self.at(f, "b", back, self.y, halves[0]))
            self.send(f"bz{f}{k + 1}", "z-", self.at(f, "b", ahead, self.y, halves[1]))

    def by(self, f, j):
        for way in ("y+", "y-"):
            self.send(f"by{f}{j}", way, self.at(f, "b", self.zi[j], self.y))

    def byf(self, f, j):
        for way, step, half in (("y+", -1, 0), ("y-", 1, 1)):
            self.got(f"by{f}{j}", way, self.at(f, "b", self.zi[j], self.yk(step)))
            self.send(f"byf{f}{j}", way, self.at(f, "b", self.zi[j], self.yk(step), half))

    def sb(self, f, j):
        for way, half in (("y+", 0), ("y-", 1)):
            self.got(f"byf{f}{j}", way, self.at(f, "b", self.zi[j], self.yk(2), half))
        self.send(f"sb{f}{j}", "s", self.at(f, "b", self.zi[j], pl.ds(0, 4)))

    def ayf(self, f):
        for way, step, half in (("y+", -1, 0), ("y-", 1, 1)):
            self.got(f"ay{f}", way, self.at(f, "a", self.z, self.yk(step)))
            self.send(f"ayf{f}", way, self.at(f, "a", self.z, self.yk(step), half))

    def sa(self, f, k):
        self.send(f"sa{f}{k}", "s", self.at(f, "a", self.zk(k), pl.ds(0, 4)))

    def az(self, f, k):
        if k == 0:
            for way, half in (("y+", 0), ("y-", 1)):
                self.got(f"ayf{f}", way, self.at(f, "a", self.z, self.yk(2), half))
        ends = (("z+", self.zk(-k), 0), ("z-", self.zk(k), 1))
        if k == 4:
            for way, zi, p in ends:
                self.got(f"az{f}4", way, self.at(f, "a", zi, pl.ds(2 * p, 2)))
            self.sa(f, 4)
            return
        for p in range(2):
            for way, zi, mine in ends:
                at = self.at(f, "a", zi, pl.ds(2 * p, 2))
                if k:
                    self.got(f"az{f}{k}{p}", way, at)
                if k < 3:
                    self.send(f"az{f}{k + 1}{p}", way, at)
                elif p == mine:
                    self.send(f"az{f}4", way, at)
        self.sa(f, -k)
        if k:
            self.sa(f, k)

    def column_b(self, f, j):
        self.got(f"sb{f}{j}", "s", self.at(f, "b", self.zi[j], pl.ds(0, 4), core=1 - self.c))

    def column_a(self, f, k):
        self.got(f"sa{f}{k}", "s", self.at(f, "a", self.zk(k), pl.ds(0, 4), core=1 - self.c))

    def slot(self, name):
        for kind, *rest in STEPS[name]:
            getattr(self, kind)(*rest)


def layer_kernel(
    q_ref,
    k_ref,
    v_ref,
    og_ref,
    ig_ref,
    fg_ref,
    hg_ref,
    wo_hbm,
    st_ref,
    gain_ref,
    wg_hbm,
    wu_hbm,
    wd_hbm,
    o_ref,
    w,
    wo,
    acc,
    hid,
    y_ref,
    small1,
    small2,
    small_l,
    small_me,
    small_t,
    s_loc,
    r1,
    pre_l,
    t_loc,
    r2,
    o3,
    r3,
    part,
    rpart,
    sq_me,
    rsq,
    yloc,
    part2,
    rpart2,
    lsem,
    ss,
    rs,
    wss,
    wrs,
):
    sp, tp = lax.axis_index("sp"), lax.axis_index("tp")
    z, g = sp // NG, lax.rem(sp, NG)
    gpeer = [lax.rem(g + r, NG) for r in range(NG)]
    gfrom = [lax.rem(g + NG - r, NG) for r in range(NG)]
    zpeer = [lax.rem(z + r, NZ) for r in range(NZ)]
    xpeer = [lax.rem(tp + r, NX) for r in range(NX)]
    xfrom = [lax.rem(tp + NX - r, NX) for r in range(NX)]
    gdev = [{"sp": z * NG + p, "tp": tp} for p in gpeer]
    zdev = [{"sp": p * NG + g, "tp": tp} for p in zpeer]
    xdev = [{"sp": sp, "tp": p} for p in xpeer]
    bar, count = barrier_all(gdev[1:] + zdev[1:] + xdev[1:])
    net = Weights(w, wss, wrs, z, g, tp)
    loads = [
        pltpu.make_async_copy(ref, w.at[kind, z, net.y, net.c], lsem.at[kind])
        for kind, ref in enumerate((wg_hbm, wu_hbm, wd_hbm))
    ]
    loads.append(pltpu.make_async_copy(wo_hbm, wo, lsem.at[3]))
    for c in loads:
        c.start()

    rows = lax.broadcasted_iota(jnp.int32, (TOK, TOK), 0)
    cols = lax.broadcasted_iota(jnp.int32, (TOK, TOK), 1)
    eye = rows == cols
    low = rows >= cols

    lf = log_sigmoid(fg_ref[...])
    ig = ig_ref[...]
    small_me[...] = jnp.zeros_like(small_me)
    cs_cols, pairs, wks = [], [], []
    for h in range(2):
        lf_row = lf[h : h + 1, :]
        lf_col = col_of(lf_row, eye)
        cs_col = jnp.sum(jnp.where(low, lf_row, 0.0), axis=1, keepdims=True)
        cs_row = jnp.sum(jnp.where(rows <= cols, lf_col, 0.0), axis=0, keepdims=True)
        ig_row = ig[h : h + 1, :]
        rest_row = ig_row - cs_row
        rest_col = col_of(rest_row, eye)
        top = jnp.max(rest_row, axis=1, keepdims=True)
        total = jnp.sum(lf_row, axis=1, keepdims=True)
        wk = jnp.exp(rest_col - top) * k_ref[:, h * DQK : (h + 1) * DQK].astype(f32)
        small_me[h : h + 1, :] = jnp.sum(wk, axis=0, keepdims=True)
        small_me[2 + h : 3 + h, :] = jnp.broadcast_to(total, (1, TOK))
        small_me[4 + h : 5 + h, :] = jnp.broadcast_to(total + top, (1, TOK))
        cs_cols.append(cs_col)
        pairs.append((rest_row, ig_row))
        wks.append(wk)
    pl.semaphore_wait(bar, count)
    pending = []
    for r in range(1, NG):
        c = copy_to(small_me, small1.at[g], ss.at[0, r], rs.at[0, r], gdev[r])
        c.start()
        pending.append(c)
    small1[g] = small_me[...]
    for c in loads[:3]:
        c.wait()
    net.slot("first")

    for h in range(2):
        hi, lo = split_hi_lo(wks[h])
        v_h = v_ref[:, h * DV : (h + 1) * DV]
        state = dot(hi, v_h, ((0,), (0,))) + dot(lo, v_h, ((0,), (0,)))
        s_loc[4 * h : 4 * h + 4] = state.astype(bf16).reshape(4, 32, DV)
    for r in range(1, NG):
        c = copy_to(s_loc.at[gpeer[r]], r1.at[g], ss.at[1, r], rs.at[1, r], gdev[r])
        c.start()
        pending.append(c)
    r1[g] = s_loc[g]
    net.slot("slices")

    scale = DQK**-0.5
    num0, den0, peak0 = [], [], []
    for h in range(2):
        rest_row, ig_row = pairs[h]
        q_h = q_ref[:, h * DQK : (h + 1) * DQK]
        k_h = k_ref[:, h * DQK : (h + 1) * DQK]
        log_pair = jnp.where(low, cs_cols[h] + rest_row, -jnp.inf)
        peak = jnp.max(log_pair, axis=1, keepdims=True)
        scores = dot(q_h, k_h, ((1,), (1,))) * scale * jnp.exp(log_pair - peak)
        hi, lo = split_hi_lo(scores)
        v_h = v_ref[:, h * DV : (h + 1) * DV]
        num0.append(dot(hi, v_h) + dot(lo, v_h))
        den0.append(jnp.sum(scores, axis=1, keepdims=True))
        peak0.append(peak)

    for r in range(1, NG):
        pltpu.make_async_remote_copy(
            small_me, small1.at[gfrom[r]], ss.at[0, r], rs.at[0, r], gdev[r], MESH
        ).wait_recv()
    n_l = jnp.zeros((2, TOK), f32)
    a_l = jnp.zeros((2, TOK), f32)
    m_l = jnp.full((2, TOK), very_low, f32)
    a_list, m_list, f_list, l_list = [], [], [], []
    for i in range(NG):
        small_l[i, 0:2, :] = n_l
        small_l[i, 2:4, :] = a_l
        small_l[i, 4:6, :] = m_l
        a_list.append(a_l)
        m_list.append(m_l)
        n_i, a_i, m_i = small1[i, 0:2, :], small1[i, 2:4, :], small1[i, 4:6, :]
        new = jnp.maximum(a_i + m_l, m_i)
        former, latter = jnp.exp(a_i + m_l - new), jnp.exp(m_i - new)
        f_list.append(former)
        l_list.append(latter)
        n_l = former * n_l + latter * n_i
        a_l = a_l + a_i
        m_l = new
    small_t[...] = jnp.zeros_like(small_t)
    small_t[0:2, :] = n_l
    small_t[2:4, :] = a_l
    small_t[4:6, :] = m_l
    for r in range(1, NZ):
        c = copy_to(small_t, small2.at[z], ss.at[2, r], rs.at[2, r], zdev[r])
        c.start()
        pending.append(c)
    small2[z] = small_t[...]

    def mine(pair):
        return jnp.where(g < 4, pair[0:1, :], pair[1:2, :])

    def spread(line):
        return jnp.concatenate([line, line], axis=1)

    for r in range(1, NG):
        copy_to(s_loc.at[0], r1.at[gfrom[r]], ss.at[1, r], rs.at[1, r], gdev[r]).wait_recv()
    run = jnp.zeros((32, DV), f32)
    for i in range(NG):
        pre_l[i] = run
        run = spread(mine(f_list[i])) * run + spread(mine(l_list[i])) * r1[i].astype(f32)
    t_loc[...] = run.astype(bf16)
    for r in range(1, NZ):
        c = copy_to(t_loc, r2.at[z], ss.at[3, r], rs.at[3, r], zdev[r])
        c.start()
        pending.append(c)
    r2[z] = t_loc[...]
    net.slot("totals")

    for r in range(1, NZ):
        copy_to(
            small_t, small2.at[lax.rem(z + NZ - r, NZ)], ss.at[2, r], rs.at[2, r], zdev[r]
        ).wait_recv()
    n_z = jnp.zeros((2, TOK), f32)
    m_z = jnp.full((2, TOK), very_low, f32)
    fz, lz = [], []
    for i in range(NZ):
        on = i < z
        n_i, a_i, m_i = small2[i, 0:2, :], small2[i, 2:4, :], small2[i, 4:6, :]
        new = jnp.maximum(a_i + m_z, m_i)
        former, latter = jnp.exp(a_i + m_z - new), jnp.exp(m_i - new)
        former = jnp.where(on, former, 1.0)
        latter = jnp.where(on, latter, 0.0)
        fz.append(mine(former))
        lz.append(mine(latter))
        n_z = former * n_z + latter * n_i
        m_z = jnp.where(on, new, m_z)
    ca, cb = [], []
    for j in range(NG):
        new = jnp.maximum(a_list[j] + m_z, m_list[j])
        ca.append(mine(jnp.exp(m_list[j] - new)))
        cb.append(mine(jnp.exp(a_list[j] + m_z - new)))
    n_g, a_g, m_g = small_l[g, 0:2, :], small_l[g, 2:4, :], small_l[g, 4:6, :]
    m_in = jnp.maximum(a_g + m_z, m_g)
    n_in = jnp.exp(m_g - m_in) * n_g + jnp.exp(a_g + m_z - m_in) * n_z

    scale0, carried, denom = [], [], []
    for h in range(2):
        q_h = q_ref[:, h * DQK : (h + 1) * DQK].astype(f32)
        log_carry = cs_cols[h] + m_in[h : h + 1, 0:1]
        peak = jnp.maximum(peak0[h], log_carry)
        s0, c0 = jnp.exp(peak0[h] - peak), jnp.exp(log_carry - peak) * scale
        normer = s0 * den0[h] + c0 * jnp.sum(q_h * n_in[h : h + 1, :], axis=1, keepdims=True)
        inv = 1.0 / jnp.maximum(jnp.abs(normer), jnp.exp(-peak))
        scale0.append(s0 * inv)
        carried.append(c0 * inv)

    for r in range(1, NZ):
        copy_to(
            t_loc, r2.at[lax.rem(z + NZ - r, NZ)], ss.at[3, r], rs.at[3, r], zdev[r]
        ).wait_recv()
    run = jnp.zeros((32, DV), f32)
    for i in range(NZ):
        run = spread(fz[i]) * run + spread(lz[i]) * r2[i].astype(f32)
    for j in range(NG):
        o3[j] = (spread(ca[j]) * pre_l[j] + spread(cb[j]) * run).astype(bf16)
    for r in range(1, NG):
        c = copy_to(o3.at[gpeer[r]], r3.at[g], ss.at[4, r], rs.at[4, r], gdev[r])
        c.start()
        pending.append(c)
    r3[g] = o3[g]
    net.slot("prefix")
    gates = [
        hg_ref[:, h * DV : (h + 1) * DV]
        / (1.0 + jnp.exp(-og_ref[:, h * DV : (h + 1) * DV].astype(f32)))
        for h in range(2)
    ]
    for r in range(1, NG):
        copy_to(o3.at[0], r3.at[gfrom[r]], ss.at[4, r], rs.at[4, r], gdev[r]).wait_recv()
    gated, sq = [], jnp.zeros((TOK, 1), f32)
    for h in range(2):
        q_h = q_ref[:, h * DQK : (h + 1) * DQK]
        state = r3[4 * h : 4 * h + 4].reshape(DQK, DV)
        out = scale0[h] * num0[h] + carried[h] * dot(q_h, state)
        sq = sq + jnp.sum(out * out, axis=1, keepdims=True)
        gated.append((out * gates[h]).astype(bf16))
    sq_me[0] = jnp.broadcast_to(row_of(sq, eye), (8, TOK))
    for r in range(1, NX):
        c = copy_to(sq_me.at[0], rsq.at[0, tp], ss.at[5, r], rs.at[5, r], xdev[r])
        c.start()
        pending.append(c)
    rsq[0, tp] = sq_me[0]
    heads = jnp.concatenate(gated, axis=1)
    loads[3].wait()
    for r in (2, 1, 3, 0):
        at = pl.multiple_of(xpeer[r] * COLS, COLS)
        part[xpeer[r]] = dot(heads, wo[:, pl.ds(at, COLS)]).astype(bf16)
        if r:
            c = copy_to(part.at[xpeer[r]], rpart.at[tp], ss.at[6, r], rs.at[6, r], xdev[r])
            c.start()
            pending.append(c)
    rpart[tp] = part[tp]
    net.slot("parts")
    for r in range(1, NX):
        copy_to(sq_me.at[0], rsq.at[0, xfrom[r]], ss.at[5, r], rs.at[5, r], xdev[r]).wait_recv()
    sq_all = jnp.sum(rsq[0, :, 0, :], axis=0, keepdims=True)
    row_scale = col_of(lax.rsqrt(sq_all / VALS + norm_eps), eye)
    for r in range(1, NX):
        copy_to(part.at[0], rpart.at[xfrom[r]], ss.at[6, r], rs.at[6, r], xdev[r]).wait_recv()
    mixer = rpart[0].astype(f32)
    for i in range(1, NX):
        mixer = mixer + rpart[i].astype(f32)
    resid = (st_ref[...].astype(f32) + mixer * row_scale).astype(bf16)
    resid_f = resid.astype(f32)
    gain = gain_ref[:, pl.ds(pl.multiple_of(tp * COLS, COLS), COLS)]
    yloc[...] = (resid_f * gain).astype(bf16)
    sq_me[1] = jnp.broadcast_to(
        row_of(jnp.sum(resid_f * resid_f, axis=1, keepdims=True), eye), (8, TOK)
    )
    for r in (2, 1, 3):
        c = copy_to(yloc, y_ref.at[tp], ss.at[8, r], rs.at[8, r], xdev[r])
        c.start()
        pending.append(c)
    for r in range(1, NX):
        c = copy_to(sq_me.at[1], rsq.at[1, tp], ss.at[7, r], rs.at[7, r], xdev[r])
        c.start()
        pending.append(c)
    rsq[1, tp] = sq_me[1]
    y_ref[tp] = yloc[...]
    net.slot("feats")
    for r in range(1, NX):
        copy_to(sq_me.at[1], rsq.at[1, xfrom[r]], ss.at[7, r], rs.at[7, r], xdev[r]).wait_recv()
    sq_all = jnp.sum(rsq[1, :, 0, :], axis=0, keepdims=True)
    scale_in = col_of(lax.rsqrt(sq_all / D + norm_eps), eye)
    for r in range(1, NX):
        copy_to(yloc, y_ref.at[xfrom[r]], ss.at[8, r], rs.at[8, r], xdev[r]).wait_recv()
    def y_col(zi):
        return y_ref[zi // 2, :, pl.ds(pl.multiple_of(lax.rem(zi, 2) * 256, 256), 256)]

    seen = set()

    def column(route, zi):
        lanes = net.lanes("u", route)
        for kind in range(2):
            term = dot(y_col(zi), w[kind, zi, :, :, :, lanes].reshape(256, lanes.size))
            if (route, kind) in seen:
                acc[kind, :, lanes] += term
            else:
                acc[kind, :, lanes] = term
            seen.add((route, kind))

    arrived = set()
    for kind, *rest in STEPS["rest"]:
        if kind == "fb":
            net.column_b(*rest)
            column("b", net.zi[rest[1]])
        elif kind == "fa":
            net.column_a(*rest)
            column("a", net.zk(rest[1]))
        elif kind == "hid":
            gate = acc[0] * scale_in
            hid[...] = (gate / (1.0 + jnp.exp(-gate)) * (acc[1] * scale_in)).astype(bf16)
        elif kind == "dn":
            for k in {0: (0, -1, 1), 1: (2, 3), 3: (-2, -3), 2: (4,)}[rest[1]]:
                net.column_b("d", COLUMNS.index(k))
                net.column_a("d", k)
            at = lax.rem(z // 2 + rest[1], NX)
            part2[at] = dot(
                hid[...], w[2, pl.ds(2 * at, 2)].reshape(COLS, FFT), ((1,), (1,))
            ).astype(bf16)

            @pl.when(at != tp)
            def _():
                r = lax.rem(at - tp + NX, NX)
                copy_to(
                    part2.at[at], rpart2.at[tp], ss.at[9, r], rs.at[9, r], {"sp": sp, "tp": at}
                ).start()
        else:
            getattr(net, kind)(*rest)
    total = resid_f + part2[tp].astype(f32)
    for r in range(1, NX):
        copy_to(part2.at[0], rpart2.at[xfrom[r]], ss.at[9, r], rs.at[9, r], xdev[r]).wait_recv()
        total = total + rpart2[xfrom[r]].astype(f32)
    o_ref[...] = total.astype(bf16)
    for r in range(1, NX):
        copy_to(part2.at[0], rpart2.at[tp], ss.at[9, r], rs.at[9, r], xdev[r]).wait_send()
    for c in pending + net.sent:
        c.wait_send()


def local(
    stream,
    queries,
    keys,
    values,
    out_gate,
    input_gate,
    forget_gate,
    head_gain,
    w_out,
    ffn_gain,
    w_gate,
    w_up,
    w_down,
):
    vmem = pl.BlockSpec(memory_space=pltpu.VMEM)
    hbm = pl.BlockSpec(memory_space=pl.ANY)
    return pl.pallas_call(
        layer_kernel,
        out_shape=jax.ShapeDtypeStruct((TOK, COLS), bf16),
        in_specs=[vmem] * 7 + [hbm] + [vmem] * 2 + [hbm] * 3,
        out_specs=vmem,
        scratch_shapes=[
            pltpu.VMEM((3, NZ, 4, 2, 32, FFT), bf16),
            pltpu.VMEM((COLS, D), bf16),
            pltpu.VMEM((2, TOK, FFT), f32),
            pltpu.VMEM((TOK, FFT), bf16),
            pltpu.VMEM((NX, TOK, COLS), bf16),
            pltpu.VMEM((NG, 8, TOK), f32),
            pltpu.VMEM((NZ, 8, TOK), f32),
            pltpu.VMEM((NG, 8, TOK), f32),
            pltpu.VMEM((8, TOK), f32),
            pltpu.VMEM((8, TOK), f32),
            pltpu.VMEM((NG, 32, DV), bf16),
            pltpu.VMEM((NG, 32, DV), bf16),
            pltpu.VMEM((NG, 32, DV), f32),
            pltpu.VMEM((32, DV), bf16),
            pltpu.VMEM((NZ, 32, DV), bf16),
            pltpu.VMEM((NG, 32, DV), bf16),
            pltpu.VMEM((NG, 32, DV), bf16),
            pltpu.VMEM((NX, TOK, COLS), bf16),
            pltpu.VMEM((NX, TOK, COLS), bf16),
            pltpu.VMEM((2, 8, TOK), f32),
            pltpu.VMEM((2, NX, 8, TOK), f32),
            pltpu.VMEM((TOK, COLS), bf16),
            pltpu.VMEM((NX, TOK, COLS), bf16),
            pltpu.VMEM((NX, TOK, COLS), bf16),
            pltpu.SemaphoreType.DMA((4,)),
            pltpu.SemaphoreType.DMA((10, 8)),
            pltpu.SemaphoreType.DMA((10, 8)),
            pltpu.SemaphoreType.DMA((160,)),
            pltpu.SemaphoreType.DMA((160,)),
        ],
        compiler_params=pltpu.CompilerParams(
            collective_id=0, has_side_effects=True, vmem_limit_bytes=60 * 2**20
        ),
    )(
        queries,
        keys,
        values,
        out_gate,
        input_gate.T,
        forget_gate.T,
        head_gain.reshape(1, COLS),
        w_out,
        stream,
        ffn_gain.reshape(1, D),
        w_gate,
        w_up,
        w_down.T,
    )


def solution(mesh):
    in_specs = (
        P("sp", "tp"),
        P("sp", "tp"),
        P("sp", "tp"),
        P("sp", "tp"),
        P("sp", "tp"),
        P("sp", "tp"),
        P("sp", "tp"),
        P("tp"),
        P("tp", None),
        P(),
        P("sp", "tp"),
        P("sp", "tp"),
        P("tp", "sp"),
    )
    return jax.shard_map(
        local, mesh=mesh, in_specs=in_specs, out_specs=P("sp", "tp"), check_vma=False
    )
```

```python
import functools

import jax
import jax.numpy as jnp
from jax import lax
from jax.experimental import pallas as pl
from jax.experimental.pallas import tpu as pltpu
from jax.sharding import PartitionSpec as P

D = 2048
DQK = 128
DV = 256
VALS = 2048
FFT = 1408
TOK = 128
COLS = 512
NG = 8
NZ = 8
NX = 4
norm_eps = 1e-06
very_low = -1e30
MESH = pl.DeviceIdType.MESH
f32 = jnp.float32
bf16 = jnp.bfloat16


def row_of(col, eye):
    return jnp.sum(jnp.where(eye, col, 0.0), axis=0, keepdims=True)


def col_of(row, eye):
    return jnp.sum(jnp.where(eye, row, 0.0), axis=1, keepdims=True)


def split_hi_lo(x):
    hi = x.astype(bf16)
    return hi, (x - hi.astype(f32)).astype(bf16)


def dot(a, b, dims=((1,), (0,))):
    return lax.dot_general(a, b, (dims, ((), ())), preferred_element_type=f32)


def log_sigmoid(x):
    return jnp.minimum(x, 0.0) - jnp.log1p(jnp.exp(-jnp.abs(x)))


def copy_to(src, dst, ssem, rsem, dev):
    return pltpu.make_async_remote_copy(
        src_ref=src, dst_ref=dst, send_sem=ssem, recv_sem=rsem, device_id=dev, device_id_type=MESH
    )


def barrier_all(devs):
    bar = pltpu.get_barrier_semaphore()
    for dev in devs:
        pl.semaphore_signal(bar, inc=1, device_id=dev, device_id_type=MESH)
    return bar, len(devs)


RING = 6
COLUMNS = (0, -1, 1, -2, 2, -3, 3, 4)
GROUPS = {0: (0, -1, 1), 1: (2, 3), 3: (-2, -3), 2: (4,)}
GROUP_OF = {k: m for m, ks in GROUPS.items() for k in ks}
SPLIT = {"u": 512, "d": 640}
STEPS = {
    "first": (
        ("own", "u"),
        ("by", "u", 0),
    ),
    "slices": (
    ),
    "totals": (
        ("ayf", "u"),
        ("bz", "u", 1),
        ("by", "u", 1),
        ("by", "u", 2),
        ("byf", "u", 0),
        ("az", "u", 0),
        ("sa", "u", 0),
        ("byf", "u", 1),
    ),
    "prefix": (
        ("own", "d"),
        ("bz", "u", 2),
        ("by", "u", 3),
        ("by", "u", 4),
        ("byf", "u", 2),
        ("sb", "u", 0),
        ("sb", "u", 1),
    ),
    "parts": (
        ("az", "u", 1),
        ("sa", "u", -1),
        ("sa", "u", 1),
        ("ayf", "d"),
        ("byf", "u", 3),
        ("bz", "d", 1),
        ("bz", "u", 3),
        ("by", "u", 5),
        ("by", "u", 6),
        ("byf", "u", 4),
        ("sb", "u", 2),
        ("az", "d", 0),
        ("sa", "d", 0),
        ("sb", "u", 3),
        ("az", "u", 2),
        ("sa", "u", -2),
    ),
    "feats": (
        ("sa", "u", 2),
        ("by", "d", 0),
        ("byf", "u", 5),
        ("bz", "u", 4),
        ("by", "u", 7),
        ("byf", "u", 6),
        ("sb", "u", 4),
        ("bz", "d", 2),
        ("az", "d", 1),
        ("sa", "d", -1),
        ("sa", "d", 1),
        ("by", "d", 1),
        ("sb", "u", 5),
    ),
    "rest": (
        ("fa", "u", -2),
        ("fa", "u", -1),
        ("fb", "u", 0),
        ("fa", "u", 0),
        ("fb", "u", 1),
        ("fa", "u", 1),
        ("fb", "u", 2),
        ("fa", "u", 2),
        ("fb", "u", 3),
        ("byf", "u", 7),
        ("fb", "u", 4),
        ("fb", "u", 5),
        ("by", "d", 2),
        ("by", "d", 3),
        ("sb", "u", 6),
        ("by", "d", 4),
        ("az", "u", 3),
        ("sa", "u", -3),
        ("sa", "u", 3),
        ("byf", "d", 0),
        ("byf", "d", 1),
        ("bz", "d", 3),
        ("fb", "u", 6),
        ("sb", "u", 7),
        ("by", "d", 5),
        ("fa", "u", -3),
        ("by", "d", 6),
        ("fa", "u", 3),
        ("byf", "d", 2),
        ("fb", "u", 7),
        ("az", "d", 2),
        ("byf", "d", 3),
        ("sa", "d", -2),
        ("sa", "d", 2),
        ("byf", "d", 4),
        ("sb", "d", 0),
        ("sb", "d", 1),
        ("byf", "d", 5),
        ("az", "u", 4),
        ("sa", "u", 4),
        ("bz", "d", 4),
        ("by", "d", 7),
        ("byf", "d", 6),
        ("sb", "d", 2),
        ("sb", "d", 3),
        ("fa", "u", 4),
        ("hid", "u"),
        ("sb", "d", 4),
        ("dn", "d", 0),
        ("sb", "d", 5),
        ("byf", "d", 7),
        ("az", "d", 3),
        ("sa", "d", -3),
        ("sa", "d", 3),
        ("sb", "d", 6),
        ("dn", "d", 3),
        ("sb", "d", 7),
        ("dn", "d", 1),
        ("az", "d", 4),
        ("sa", "d", 4),
        ("dn", "d", 2),
    ),
}


class Weights:
    def __init__(self, bufs, ssem, rsem, z, g, tp):
        self.bufs, self.ssem, self.rsem = bufs, ssem, rsem
        self.z, self.y, self.c, self.tp = z, g // 2, lax.rem(g, 2), tp
        self.ids, self.sent = {}, {}
        self.zi = [self.zk(k) for k in COLUMNS]

        def z_at(k):
            return {"sp": lax.rem(z + k, NZ) * NG + g, "tp": tp}

        def y_at(k):
            return {"sp": z * NG + lax.rem(self.y + k, 4) * 2 + self.c, "tp": tp}

        self.dev = {
            "z+": z_at(1),
            "z-": z_at(7),
            "y+": y_at(1),
            "y-": y_at(3),
            "s": {"sp": z * NG + self.y * 2 + (1 - self.c), "tp": tp},
        }
        self.ways = list(self.dev)

    def zk(self, k):
        return lax.rem(self.z + NZ + k, NZ)

    def yk(self, k):
        return lax.rem(self.y + 4 + k, 4)

    def at(self, f, route, zi, yi, half=None, core=None):
        kinds, rows = pl.ds(0, 2 if f == "u" else 1), pl.ds(0, 32)
        if half is not None:
            kinds, rows = (pl.ds(half, 1), rows) if f == "u" else (kinds, pl.ds(16 * half, 16))
        zs = zi if isinstance(zi, pl.Slice) else pl.ds(zi, 1)
        ys = yi if isinstance(yi, pl.Slice) else pl.ds(yi, 1)
        return self.bufs[f, route].at[kinds, zs, self.c if core is None else core, ys, rows]

    def send(self, name, way, ref):
        n = self.ids.setdefault(name, len(self.ids))
        past = self.sent.setdefault(way, [])
        k = len(past)
        if k >= RING:
            past[k - RING].wait_send()
        slot = self.ways.index(way) * RING + k % RING
        c = copy_to(ref, ref, self.ssem.at[slot], self.rsem.at[n], self.dev[way])
        c.start()
        past.append(c)

    def got(self, name, ref):
        n = self.ids.setdefault(name, len(self.ids))
        copy_to(ref, ref, self.ssem.at[0], self.rsem.at[n], self.dev["s"]).wait_recv()

    def drain(self):
        for past in self.sent.values():
            for c in past[-RING:]:
                c.wait_send()

    def own(self, f):
        for way in ("z+", "z-"):
            self.send(f"bz{f}1", way, self.at(f, "b", self.z, self.y))
        for way in ("y+", "y-"):
            self.send(f"ay{f}", way, self.at(f, "a", self.z, self.y))

    def bz(self, f, k):
        self.got(f"bz{f}{k}", self.at(f, "b", pl.ds(0, 1 if k == 4 else 2), self.y))
        if k < 4:
            halves = (0, 1) if k == 3 else (None, None)
            self.send(f"bz{f}{k + 1}", "z+", self.at(f, "b", self.zk(-k), self.y, halves[0]))
            self.send(f"bz{f}{k + 1}", "z-", self.at(f, "b", self.zk(k), self.y, halves[1]))

    def by(self, f, j):
        for way in ("y+", "y-"):
            self.send(f"by{f}{j}", way, self.at(f, "b", self.zi[j], self.y))

    def byf(self, f, j):
        self.got(f"by{f}{j}", self.at(f, "b", self.zi[j], pl.ds(0, 2)))
        self.send(f"byf{f}{j}", "y+", self.at(f, "b", self.zi[j], self.yk(-1), 0))
        self.send(f"byf{f}{j}", "y-", self.at(f, "b", self.zi[j], self.yk(1), 1))

    def sb(self, f, j):
        self.got(f"byf{f}{j}", self.at(f, "b", self.zi[j], self.yk(2)))
        group = j if f == "u" else GROUP_OF[COLUMNS[j]]
        self.send(f"sb{f}{group}", "s", self.at(f, "b", self.zi[j], pl.ds(0, 4)))

    def ayf(self, f):
        self.got(f"ay{f}", self.at(f, "a", self.z, pl.ds(0, 2)))
        self.send(f"ayf{f}", "y+", self.at(f, "a", self.z, self.yk(-1), 0))
        self.send(f"ayf{f}", "y-", self.at(f, "a", self.z, self.yk(1), 1))

    def sa(self, f, k):
        group = k if f == "u" else GROUP_OF[k]
        self.send(f"sa{f}{group}", "s", self.at(f, "a", self.zk(k), pl.ds(0, 4)))

    def az(self, f, k):
        if k == 0:
            self.got(f"ayf{f}", self.at(f, "a", self.z, self.yk(2)))
        else:
            self.got(f"az{f}{k}", self.at(f, "a", pl.ds(0, 1 if k == 4 else 2), pl.ds(0, 4)))
        if k == 4:
            return
        for p in range(2):
            for way, zi, mine in (("z+", self.zk(-k), 0), ("z-", self.zk(k), 1)):
                if k < 3 or p == mine:
                    self.send(f"az{f}{k + 1}", way, self.at(f, "a", zi, pl.ds(2 * p, 2)))

    def column_b(self, j):
        self.got(f"sbu{j}", self.at("u", "b", self.zi[j], pl.ds(0, 4)))

    def column_a(self, k):
        self.got(f"sau{k}", self.at("u", "a", self.zk(k), pl.ds(0, 4)))

    def columns_down(self, m):
        for route in "ab":
            self.got(f"s{route}d{m}", self.at("d", route, pl.ds(0, len(GROUPS[m])), pl.ds(0, 4)))

    def slot(self, name):
        for kind, *rest in STEPS[name]:
            getattr(self, kind)(*rest)


def layer_kernel(
    q_ref,
    k_ref,
    v_ref,
    og_ref,
    ig_ref,
    fg_ref,
    hg_ref,
    wo_hbm,
    st_ref,
    gain_ref,
    wg_hbm,
    wu_hbm,
    wd_hbm,
    o_ref,
    ua,
    ub,
    da,
    db,
    wo,
    acc,
    hid,
    y_ref,
    small1,
    small2,
    small_l,
    small_me,
    small_t,
    s_loc,
    r1,
    pre_l,
    t_loc,
    r2,
    o3,
    r3,
    part,
    rpart,
    sq_me,
    rsq,
    yloc,
    part2,
    rpart2,
    lsem,
    ss,
    rs,
    wss,
    wrs,
):
    sp, tp = lax.axis_index("sp"), lax.axis_index("tp")
    z, g = sp // NG, lax.rem(sp, NG)
    gpeer = [lax.rem(g + r, NG) for r in range(NG)]
    gfrom = [lax.rem(g + NG - r, NG) for r in range(NG)]
    zpeer = [lax.rem(z + r, NZ) for r in range(NZ)]
    xpeer = [lax.rem(tp + r, NX) for r in range(NX)]
    xfrom = [lax.rem(tp + NX - r, NX) for r in range(NX)]
    gdev = [{"sp": z * NG + p, "tp": tp} for p in gpeer]
    zdev = [{"sp": p * NG + g, "tp": tp} for p in zpeer]
    xdev = [{"sp": sp, "tp": p} for p in xpeer]
    def joint(n, ref):
        return copy_to(ref, ref, ss.at[n], rs.at[n], gdev[1])

    bar, count = barrier_all(gdev[1:] + zdev[1:] + xdev[1:])
    bufs = {("u", "a"): ua, ("u", "b"): ub, ("d", "a"): da, ("d", "b"): db}
    net = Weights(bufs, wss, wrs, z, g, tp)
    loads = []
    for f, kind, ref in (("u", 0, wg_hbm), ("u", 1, wu_hbm), ("d", 0, wd_hbm)):
        cut = SPLIT[f]
        for route, lanes in (("a", pl.ds(0, cut)), ("b", pl.ds(cut, FFT - cut))):
            loads.append(
                pltpu.make_async_copy(
                    ref.at[:, lanes], bufs[f, route].at[kind, z, net.c, net.y], lsem.at[len(loads)]
                )
            )
    loads.append(pltpu.make_async_copy(wo_hbm, wo, lsem.at[6]))
    for c in loads:
        c.start()
    rows = lax.broadcasted_iota(jnp.int32, (TOK, TOK), 0)
    cols = lax.broadcasted_iota(jnp.int32, (TOK, TOK), 1)
    eye = rows == cols
    low = rows >= cols

    lf = log_sigmoid(fg_ref[...])
    ig = ig_ref[...]
    small_me[...] = jnp.zeros_like(small_me)
    cs_cols, pairs, wks = [], [], []
    for h in range(2):
        lf_row = lf[h : h + 1, :]
        lf_col = col_of(lf_row, eye)
        cs_col = jnp.sum(jnp.where(low, lf_row, 0.0), axis=1, keepdims=True)
        cs_row = jnp.sum(jnp.where(rows <= cols, lf_col, 0.0), axis=0, keepdims=True)
        ig_row = ig[h : h + 1, :]
        rest_row = ig_row - cs_row
        rest_col = col_of(rest_row, eye)
        top = jnp.max(rest_row, axis=1, keepdims=True)
        total = jnp.sum(lf_row, axis=1, keepdims=True)
        wk = jnp.exp(rest_col - top) * k_ref[:, h * DQK : (h + 1) * DQK].astype(f32)
        small_me[h : h + 1, :] = jnp.sum(wk, axis=0, keepdims=True)
        small_me[2 + h : 3 + h, :] = jnp.broadcast_to(total, (1, TOK))
        small_me[4 + h : 5 + h, :] = jnp.broadcast_to(total + top, (1, TOK))
        cs_cols.append(cs_col)
        pairs.append((rest_row, ig_row))
        wks.append(wk)
    for h in range(2):
        hi, lo = split_hi_lo(wks[h])
        v_h = v_ref[:, h * DV : (h + 1) * DV]
        state = dot(hi, v_h, ((0,), (0,))) + dot(lo, v_h, ((0,), (0,)))
        s_loc[4 * h : 4 * h + 4] = state.astype(bf16).reshape(4, 32, DV)
    scale = DQK**-0.5
    num0, den0, peak0 = [], [], []
    for h in range(2):
        rest_row, ig_row = pairs[h]
        q_h = q_ref[:, h * DQK : (h + 1) * DQK]
        k_h = k_ref[:, h * DQK : (h + 1) * DQK]
        log_pair = jnp.where(low, cs_cols[h] + rest_row, -jnp.inf)
        peak = jnp.max(log_pair, axis=1, keepdims=True)
        scores = dot(q_h, k_h, ((1,), (1,))) * scale * jnp.exp(log_pair - peak)
        hi, lo = split_hi_lo(scores)
        v_h = v_ref[:, h * DV : (h + 1) * DV]
        num0.append(dot(hi, v_h) + dot(lo, v_h))
        den0.append(jnp.sum(scores, axis=1, keepdims=True))
        peak0.append(peak)

    pl.semaphore_wait(bar, count)
    for r in range(1, NG):
        copy_to(small_me, small1.at[g], ss.at[0], rs.at[0], gdev[r]).start()
        copy_to(s_loc.at[gpeer[r]], r1.at[g], ss.at[1], rs.at[1], gdev[r]).start()
    for c in loads[:6]:
        c.wait()
    net.slot("first")
    small1[g] = small_me[...]
    r1[g] = s_loc[g]
    net.slot("slices")
    joint(0, small1.at[pl.ds(0, NG - 1)]).wait_recv()
    n_l = jnp.zeros((2, TOK), f32)
    a_l = jnp.zeros((2, TOK), f32)
    m_l = jnp.full((2, TOK), very_low, f32)
    a_list, m_list, f_list, l_list = [], [], [], []
    for i in range(NG):
        small_l[i, 0:2, :] = n_l
        small_l[i, 2:4, :] = a_l
        small_l[i, 4:6, :] = m_l
        a_list.append(a_l)
        m_list.append(m_l)
        n_i, a_i, m_i = small1[i, 0:2, :], small1[i, 2:4, :], small1[i, 4:6, :]
        new = jnp.maximum(a_i + m_l, m_i)
        former, latter = jnp.exp(a_i + m_l - new), jnp.exp(m_i - new)
        f_list.append(former)
        l_list.append(latter)
        n_l = former * n_l + latter * n_i
        a_l = a_l + a_i
        m_l = new
    small_t[...] = jnp.zeros_like(small_t)
    small_t[0:2, :] = n_l
    small_t[2:4, :] = a_l
    small_t[4:6, :] = m_l
    for r in range(1, NZ):
        copy_to(small_t, small2.at[z], ss.at[2], rs.at[2], zdev[r]).start()
    small2[z] = small_t[...]

    def mine(pair):
        return jnp.where(g < 4, pair[0:1, :], pair[1:2, :])

    def spread(line):
        return jnp.concatenate([line, line], axis=1)

    joint(1, r1.at[pl.ds(0, NG - 1)]).wait_recv()
    run = jnp.zeros((32, DV), f32)
    for i in range(NG):
        pre_l[i] = run
        run = spread(mine(f_list[i])) * run + spread(mine(l_list[i])) * r1[i].astype(f32)
    t_loc[...] = run.astype(bf16)
    for r in range(1, NZ):
        copy_to(t_loc, r2.at[z], ss.at[3], rs.at[3], zdev[r]).start()
    r2[z] = t_loc[...]
    net.slot("totals")

    joint(2, small2.at[pl.ds(0, NZ - 1)]).wait_recv()
    n_z = jnp.zeros((2, TOK), f32)
    m_z = jnp.full((2, TOK), very_low, f32)
    fz, lz = [], []
    for i in range(NZ):
        on = i < z
        n_i, a_i, m_i = small2[i, 0:2, :], small2[i, 2:4, :], small2[i, 4:6, :]
        new = jnp.maximum(a_i + m_z, m_i)
        former, latter = jnp.exp(a_i + m_z - new), jnp.exp(m_i - new)
        former = jnp.where(on, former, 1.0)
        latter = jnp.where(on, latter, 0.0)
        fz.append(mine(former))
        lz.append(mine(latter))
        n_z = former * n_z + latter * n_i
        m_z = jnp.where(on, new, m_z)
    ca, cb = [], []
    for j in range(NG):
        new = jnp.maximum(a_list[j] + m_z, m_list[j])
        ca.append(mine(jnp.exp(m_list[j] - new)))
        cb.append(mine(jnp.exp(a_list[j] + m_z - new)))
    n_g, a_g, m_g = small_l[g, 0:2, :], small_l[g, 2:4, :], small_l[g, 4:6, :]
    m_in = jnp.maximum(a_g + m_z, m_g)
    n_in = jnp.exp(m_g - m_in) * n_g + jnp.exp(a_g + m_z - m_in) * n_z

    scale0, carried, denom = [], [], []
    for h in range(2):
        q_h = q_ref[:, h * DQK : (h + 1) * DQK].astype(f32)
        log_carry = cs_cols[h] + m_in[h : h + 1, 0:1]
        peak = jnp.maximum(peak0[h], log_carry)
        s0, c0 = jnp.exp(peak0[h] - peak), jnp.exp(log_carry - peak) * scale
        normer = s0 * den0[h] + c0 * jnp.sum(q_h * n_in[h : h + 1, :], axis=1, keepdims=True)
        inv = 1.0 / jnp.maximum(jnp.abs(normer), jnp.exp(-peak))
        scale0.append(s0 * inv)
        carried.append(c0 * inv)

    joint(3, r2.at[pl.ds(0, NZ - 1)]).wait_recv()
    run = jnp.zeros((32, DV), f32)
    for i in range(NZ):
        run = spread(fz[i]) * run + spread(lz[i]) * r2[i].astype(f32)
    for j in range(NG):
        o3[j] = (spread(ca[j]) * pre_l[j] + spread(cb[j]) * run).astype(bf16)
    for r in range(1, NG):
        copy_to(o3.at[gpeer[r]], r3.at[g], ss.at[4], rs.at[4], gdev[r]).start()
    r3[g] = o3[g]
    net.slot("prefix")
    gates = [
        hg_ref[:, h * DV : (h + 1) * DV]
        / (1.0 + jnp.exp(-og_ref[:, h * DV : (h + 1) * DV].astype(f32)))
        for h in range(2)
    ]
    joint(4, r3.at[pl.ds(0, NG - 1)]).wait_recv()
    gated, sq = [], jnp.zeros((TOK, 1), f32)
    for h in range(2):
        q_h = q_ref[:, h * DQK : (h + 1) * DQK]
        state = r3[4 * h : 4 * h + 4].reshape(DQK, DV)
        out = scale0[h] * num0[h] + carried[h] * dot(q_h, state)
        sq = sq + jnp.sum(out * out, axis=1, keepdims=True)
        gated.append((out * gates[h]).astype(bf16))
    sq_me[0] = jnp.broadcast_to(row_of(sq, eye), (8, TOK))
    for r in range(1, NX):
        copy_to(sq_me.at[0], rsq.at[0, tp], ss.at[5], rs.at[5], xdev[r]).start()
    rsq[0, tp] = sq_me[0]
    heads = jnp.concatenate(gated, axis=1)
    loads[6].wait()
    for r in (2, 1, 3, 0):
        at = pl.multiple_of(xpeer[r] * COLS, COLS)
        part[xpeer[r]] = dot(heads, wo[:, pl.ds(at, COLS)]).astype(bf16)
        if r:
            copy_to(part.at[xpeer[r]], rpart.at[tp], ss.at[6], rs.at[6], xdev[r]).start()
    rpart[tp] = part[tp]
    net.slot("parts")
    joint(5, rsq.at[0, pl.ds(0, NX - 1)]).wait_recv()
    sq_all = jnp.sum(rsq[0, :, 0, :], axis=0, keepdims=True)
    row_scale = col_of(lax.rsqrt(sq_all / VALS + norm_eps), eye)
    joint(6, rpart.at[pl.ds(0, NX - 1)]).wait_recv()
    mixer = rpart[0].astype(f32)
    for i in range(1, NX):
        mixer = mixer + rpart[i].astype(f32)
    resid = (st_ref[...].astype(f32) + mixer * row_scale).astype(bf16)
    resid_f = resid.astype(f32)
    gain = gain_ref[:, pl.ds(pl.multiple_of(tp * COLS, COLS), COLS)]
    yloc[...] = (resid_f * gain).astype(bf16)
    sq_me[1] = jnp.broadcast_to(
        row_of(jnp.sum(resid_f * resid_f, axis=1, keepdims=True), eye), (8, TOK)
    )
    for r in (2, 1, 3):
        copy_to(yloc, y_ref.at[tp], ss.at[8], rs.at[8], xdev[r]).start()
    for r in range(1, NX):
        copy_to(sq_me.at[1], rsq.at[1, tp], ss.at[7], rs.at[7], xdev[r]).start()
    rsq[1, tp] = sq_me[1]
    y_ref[tp] = yloc[...]
    net.slot("feats")
    joint(7, rsq.at[1, pl.ds(0, NX - 1)]).wait_recv()
    sq_all = jnp.sum(rsq[1, :, 0, :], axis=0, keepdims=True)
    scale_in = col_of(lax.rsqrt(sq_all / D + norm_eps), eye)
    joint(8, y_ref.at[pl.ds(0, NX - 1)]).wait_recv()
    def y_col(zi):
        return y_ref[zi // 2, :, pl.ds(pl.multiple_of(lax.rem(zi, 2) * 256, 256), 256)]

    seen = set()

    def rows_of(f, route, kind, zi):
        buf = bufs[f, route]
        return [buf[kind, zi, core, yi] for yi in range(4) for core in range(2)]

    def column(route, zi):
        cut = SPLIT["u"]
        lanes = pl.ds(0, cut) if route == "a" else pl.ds(cut, FFT - cut)
        for kind in range(2):
            term = dot(y_col(zi), jnp.concatenate(rows_of("u", route, kind, zi), axis=0))
            if (route, kind) in seen:
                acc[kind, :, lanes] += term
            else:
                acc[kind, :, lanes] = term
            seen.add((route, kind))

    for kind, *rest in STEPS["rest"]:
        if kind == "fb":
            net.column_b(rest[1])
            column("b", net.zi[rest[1]])
        elif kind == "fa":
            net.column_a(rest[1])
            column("a", net.zk(rest[1]))
        elif kind == "hid":
            gate = acc[0] * scale_in
            hid[...] = (gate / (1.0 + jnp.exp(-gate)) * (acc[1] * scale_in)).astype(bf16)
        elif kind == "dn":
            net.columns_down(rest[1])
            at = lax.rem(z // 2 + rest[1], NX)
            cut = SPLIT["d"]
            term = jnp.zeros((TOK, COLS), f32)
            for route, lanes in (("a", pl.ds(0, cut)), ("b", pl.ds(cut, FFT - cut))):
                rows_d = rows_of("d", route, 0, 2 * at) + rows_of("d", route, 0, 2 * at + 1)
                term = term + dot(hid[:, lanes], jnp.concatenate(rows_d, axis=0), ((1,), (1,)))
            part2[at] = term.astype(bf16)

            @pl.when(at != tp)
            def _():
                copy_to(
                    part2.at[at], rpart2.at[tp], ss.at[9], rs.at[9], {"sp": sp, "tp": at}
                ).start()
        else:
            getattr(net, kind)(*rest)
    total = resid_f + part2[tp].astype(f32)
    joint(9, rpart2.at[pl.ds(0, NX - 1)]).wait_recv()
    for r in range(1, NX):
        total = total + rpart2[xfrom[r]].astype(f32)
    o_ref[...] = total.astype(bf16)
    for n, ref in enumerate(
        (
            small1.at[pl.ds(0, NG - 1)],
            r1.at[pl.ds(0, NG - 1)],
            small2.at[pl.ds(0, NZ - 1)],
            r2.at[pl.ds(0, NZ - 1)],
            r3.at[pl.ds(0, NG - 1)],
            rsq.at[0, pl.ds(0, NX - 1)],
            rpart.at[pl.ds(0, NX - 1)],
            rsq.at[1, pl.ds(0, NX - 1)],
            y_ref.at[pl.ds(0, NX - 1)],
            rpart2.at[pl.ds(0, NX - 1)],
        )
    ):
        joint(n, ref).wait_send()
    net.drain()


def local(
    stream,
    queries,
    keys,
    values,
    out_gate,
    input_gate,
    forget_gate,
    head_gain,
    w_out,
    ffn_gain,
    w_gate,
    w_up,
    w_down,
):
    vmem = pl.BlockSpec(memory_space=pltpu.VMEM)
    hbm = pl.BlockSpec(memory_space=pl.ANY)
    return pl.pallas_call(
        layer_kernel,
        out_shape=jax.ShapeDtypeStruct((TOK, COLS), bf16),
        in_specs=[vmem] * 7 + [hbm] + [vmem] * 2 + [hbm] * 3,
        out_specs=vmem,
        scratch_shapes=[
            pltpu.VMEM((2, NZ, 2, 4, 32, SPLIT["u"]), bf16),
            pltpu.VMEM((2, NZ, 2, 4, 32, FFT - SPLIT["u"]), bf16),
            pltpu.VMEM((1, NZ, 2, 4, 32, SPLIT["d"]), bf16),
            pltpu.VMEM((1, NZ, 2, 4, 32, FFT - SPLIT["d"]), bf16),
            pltpu.VMEM((COLS, D), bf16),
            pltpu.VMEM((2, TOK, FFT), f32),
            pltpu.VMEM((TOK, FFT), bf16),
            pltpu.VMEM((NX, TOK, COLS), bf16),
            pltpu.VMEM((NG, 8, TOK), f32),
            pltpu.VMEM((NZ, 8, TOK), f32),
            pltpu.VMEM((NG, 8, TOK), f32),
            pltpu.VMEM((8, TOK), f32),
            pltpu.VMEM((8, TOK), f32),
            pltpu.VMEM((NG, 32, DV), bf16),
            pltpu.VMEM((NG, 32, DV), bf16),
            pltpu.VMEM((NG, 32, DV), f32),
            pltpu.VMEM((32, DV), bf16),
            pltpu.VMEM((NZ, 32, DV), bf16),
            pltpu.VMEM((NG, 32, DV), bf16),
            pltpu.VMEM((NG, 32, DV), bf16),
            pltpu.VMEM((NX, TOK, COLS), bf16),
            pltpu.VMEM((NX, TOK, COLS), bf16),
            pltpu.VMEM((2, 8, TOK), f32),
            pltpu.VMEM((2, NX, 8, TOK), f32),
            pltpu.VMEM((TOK, COLS), bf16),
            pltpu.VMEM((NX, TOK, COLS), bf16),
            pltpu.VMEM((NX, TOK, COLS), bf16),
            pltpu.SemaphoreType.DMA((7,)),
            pltpu.SemaphoreType.DMA((10,)),
            pltpu.SemaphoreType.DMA((10,)),
            pltpu.SemaphoreType.DMA((5 * RING,)),
            pltpu.SemaphoreType.DMA((76,)),
        ],
        compiler_params=pltpu.CompilerParams(
            collective_id=0, has_side_effects=True, vmem_limit_bytes=60 * 2**20
        ),
    )(
        queries,
        keys,
        values,
        out_gate,
        input_gate.T,
        forget_gate.T,
        head_gain.reshape(1, COLS),
        w_out,
        stream,
        ffn_gain.reshape(1, D),
        w_gate,
        w_up,
        w_down.T,
    )


def solution(mesh):
    in_specs = (
        P("sp", "tp"),
        P("sp", "tp"),
        P("sp", "tp"),
        P("sp", "tp"),
        P("sp", "tp"),
        P("sp", "tp"),
        P("sp", "tp"),
        P("tp"),
        P("tp", None),
        P(),
        P("sp", "tp"),
        P("sp", "tp"),
        P("tp", "sp"),
    )
    return jax.shard_map(
        local, mesh=mesh, in_specs=in_specs, out_specs=P("sp", "tp"), check_vma=False
    )
```

```python
import functools

import jax
import jax.numpy as jnp
from jax import lax
from jax.experimental import pallas as pl
from jax.experimental.pallas import tpu as pltpu
from jax.sharding import PartitionSpec as P

D = 2048
DQK = 128
DV = 256
VALS = 2048
FFT = 1408
TOK = 128
COLS = 512
NG = 8
NZ = 8
NX = 4
norm_eps = 1e-06
very_low = -1e30
MESH = pl.DeviceIdType.MESH
f32 = jnp.float32
bf16 = jnp.bfloat16


def row_of(col, eye):
    return jnp.sum(jnp.where(eye, col, 0.0), axis=0, keepdims=True)


def col_of(row, eye):
    return jnp.sum(jnp.where(eye, row, 0.0), axis=1, keepdims=True)


def split_hi_lo(x):
    hi = x.astype(bf16)
    return hi, (x - hi.astype(f32)).astype(bf16)


def dot(a, b, dims=((1,), (0,))):
    return lax.dot_general(a, b, (dims, ((), ())), preferred_element_type=f32)


def log_sigmoid(x):
    return jnp.minimum(x, 0.0) - jnp.log1p(jnp.exp(-jnp.abs(x)))


def copy_to(src, dst, ssem, rsem, dev):
    return pltpu.make_async_remote_copy(
        src_ref=src, dst_ref=dst, send_sem=ssem, recv_sem=rsem, device_id=dev, device_id_type=MESH
    )


def barrier_all(devs):
    bar = pltpu.get_barrier_semaphore()
    for dev in devs:
        pl.semaphore_signal(bar, inc=1, device_id=dev, device_id_type=MESH)
    return bar, len(devs)


RING = 6
COLUMNS = (0, -1, 1, -2, 2, -3, 3, 4)
SPLIT = {"u": 512, "d": 640}
STEPS = {
    "first": (
        ("own", "d"),
    ),
    "gates": (
    ),
    "slices": (
        ("own", "u"),
        ("by", "d", 0),
        ("bz", "d", 1),
        ("by", "d", 2),
        ("by", "d", 1),
    ),
    "totals": (
        ("ayf", "u"),
        ("byf", "d", 0),
        ("ayf", "d"),
        ("bz", "u", 1),
        ("by", "u", 0),
        ("by", "u", 2),
        ("byf", "d", 1),
        ("az", "u", 0),
        ("bz", "u", 2),
    ),
    "prefix": (
        ("bz", "d", 2),
        ("by", "u", 4),
        ("by", "u", 3),
        ("by", "u", 1),
        ("az", "u", 1),
        ("az", "d", 0),
    ),
    "parts": (
        ("sb", "d", 0),
        ("bz", "u", 3),
        ("by", "u", 5),
        ("sb", "d", 1),
        ("byf", "u", 3),
        ("sa", "u", 0),
        ("byf", "u", 4),
        ("sa", "d", 0),
        ("byf", "u", 1),
        ("sa", "u", 1),
    ),
    "feats": (
        ("az", "u", 2),
        ("byf", "u", 0),
        ("byf", "u", 2),
        ("sa", "u", 2),
        ("sb", "u", 3),
        ("byf", "u", 5),
        ("sa", "u", -1),
        ("az", "d", 1),
        ("sb", "u", 4),
        ("by", "u", 6),
        ("sb", "u", 1),
        ("bz", "u", 4),
        ("sb", "u", 2),
        ("byf", "d", 2),
        ("by", "u", 7),
        ("by", "d", 4),
        ("sb", "u", 0),
        ("sb", "u", 5),
        ("sa", "d", -1),
        ("sb", "d", 2),
        ("az", "u", 3),
    ),
    "rest": (
        ("byf", "u", 6),
        ("fb", "u", 2),
        ("fa", "u", -1),
        ("sa", "u", -3),
        ("fb", "u", 3),
        ("byf", "u", 7),
        ("bz", "d", 3),
        ("by", "d", 6),
        ("fa", "u", 1),
        ("fb", "u", 5),
        ("sa", "u", 3),
        ("by", "d", 3),
        ("sa", "u", -2),
        ("fa", "u", 3),
        ("az", "d", 2),
        ("sb", "u", 6),
        ("fb", "u", 0),
        ("by", "d", 5),
        ("sb", "u", 7),
        ("fa", "u", 2),
        ("fb", "u", 4),
        ("fb", "u", 6),
        ("byf", "d", 4),
        ("az", "u", 4),
        ("sa", "u", 4),
        ("sa", "d", 1),
        ("sa", "d", -2),
        ("bz", "d", 4),
        ("fa", "u", 0),
        ("by", "d", 7),
        ("fb", "u", 1),
        ("sa", "d", 2),
        ("fa", "u", -2),
        ("fb", "u", 7),
        ("byf", "d", 3),
        ("fa", "u", 4),
        ("fa", "u", -3),
        ("byf", "d", 5),
        ("hid", "u"),
        ("byf", "d", 6),
        ("dn", "d", -1),
        ("sb", "d", 4),
        ("dn", "d", 1),
        ("az", "d", 3),
        ("byf", "d", 7),
        ("sa", "d", -3),
        ("dn", "d", 2),
        ("sb", "d", 3),
        ("sa", "d", 3),
        ("sb", "d", 5),
        ("dn", "d", 0),
        ("sb", "d", 6),
        ("dn", "d", -2),
        ("sb", "d", 7),
        ("dn", "d", -3),
        ("az", "d", 4),
        ("sa", "d", 4),
        ("dn", "d", 3),
        ("dn", "d", 4),
    ),
}


class Weights:
    def __init__(self, bufs, ssem, rsem, z, g, tp):
        self.bufs, self.ssem, self.rsem = bufs, ssem, rsem
        self.z, self.y, self.c, self.tp = z, g // 2, lax.rem(g, 2), tp
        self.ids, self.sent = {}, {}
        self.zi = [self.zk(k) for k in COLUMNS]

        def z_at(k):
            return {"sp": lax.rem(z + k, NZ) * NG + g, "tp": tp}

        def y_at(k):
            return {"sp": z * NG + lax.rem(self.y + k, 4) * 2 + self.c, "tp": tp}

        self.dev = {
            "z+": z_at(1),
            "z-": z_at(7),
            "y+": y_at(1),
            "y-": y_at(3),
            "s": {"sp": z * NG + self.y * 2 + (1 - self.c), "tp": tp},
        }
        self.ways = list(self.dev)

    def zk(self, k):
        return lax.rem(self.z + NZ + k, NZ)

    def yk(self, k):
        return lax.rem(self.y + 4 + k, 4)

    def at(self, f, route, zi, yi, half=None, core=None):
        kinds, rows = pl.ds(0, 2 if f == "u" else 1), pl.ds(0, 32)
        if half is not None:
            kinds, rows = (pl.ds(half, 1), rows) if f == "u" else (kinds, pl.ds(16 * half, 16))
        zs = zi if isinstance(zi, pl.Slice) else pl.ds(zi, 1)
        ys = yi if isinstance(yi, pl.Slice) else pl.ds(yi, 1)
        return self.bufs[f, route].at[kinds, zs, self.c if core is None else core, ys, rows]

    def send(self, name, way, ref):
        n = self.ids.setdefault(name, len(self.ids))
        past = self.sent.setdefault(way, [])
        k = len(past)
        if k >= RING:
            past[k - RING].wait_send()
        slot = self.ways.index(way) * RING + k % RING
        c = copy_to(ref, ref, self.ssem.at[slot], self.rsem.at[n], self.dev[way])
        c.start()
        past.append(c)

    def got(self, name, ref):
        n = self.ids.setdefault(name, len(self.ids))
        copy_to(ref, ref, self.ssem.at[0], self.rsem.at[n], self.dev["s"]).wait_recv()

    def drain(self):
        for past in self.sent.values():
            for c in past[-RING:]:
                c.wait_send()

    def own(self, f):
        for way in ("z+", "z-"):
            self.send(f"bz{f}1", way, self.at(f, "b", self.z, self.y))
        for way in ("y+", "y-"):
            self.send(f"ay{f}", way, self.at(f, "a", self.z, self.y))

    def bz(self, f, k):
        self.got(f"bz{f}{k}", self.at(f, "b", pl.ds(0, 1 if k == 4 else 2), self.y))
        if k < 4:
            halves = (0, 1) if k == 3 else (None, None)
            self.send(f"bz{f}{k + 1}", "z+", self.at(f, "b", self.zk(-k), self.y, halves[0]))
            self.send(f"bz{f}{k + 1}", "z-", self.at(f, "b", self.zk(k), self.y, halves[1]))

    def by(self, f, j):
        for way in ("y+", "y-"):
            self.send(f"by{f}{j}", way, self.at(f, "b", self.zi[j], self.y))

    def byf(self, f, j):
        self.got(f"by{f}{j}", self.at(f, "b", self.zi[j], pl.ds(0, 2)))
        self.send(f"byf{f}{j}", "y+", self.at(f, "b", self.zi[j], self.yk(-1), 0))
        self.send(f"byf{f}{j}", "y-", self.at(f, "b", self.zi[j], self.yk(1), 1))

    def sb(self, f, j):
        self.got(f"byf{f}{j}", self.at(f, "b", self.zi[j], self.yk(2)))
        self.send(f"sb{f}{j}", "s", self.at(f, "b", self.zi[j], pl.ds(0, 4)))

    def ayf(self, f):
        self.got(f"ay{f}", self.at(f, "a", self.z, pl.ds(0, 2)))
        self.send(f"ayf{f}", "y+", self.at(f, "a", self.z, self.yk(-1), 0))
        self.send(f"ayf{f}", "y-", self.at(f, "a", self.z, self.yk(1), 1))

    def sa(self, f, k):
        self.send(f"sa{f}{k}", "s", self.at(f, "a", self.zk(k), pl.ds(0, 4)))

    def az(self, f, k):
        if k == 0:
            self.got(f"ayf{f}", self.at(f, "a", self.z, self.yk(2)))
        else:
            self.got(f"az{f}{k}", self.at(f, "a", pl.ds(0, 1 if k == 4 else 2), pl.ds(0, 4)))
        if k == 4:
            return
        for p in range(2):
            for way, zi, mine in (("z+", self.zk(-k), 0), ("z-", self.zk(k), 1)):
                if k < 3 or p == mine:
                    self.send(f"az{f}{k + 1}", way, self.at(f, "a", zi, pl.ds(2 * p, 2)))

    def column_b(self, f, j):
        self.got(f"sb{f}{j}", self.at(f, "b", self.zi[j], pl.ds(0, 4)))

    def column_a(self, f, k):
        self.got(f"sa{f}{k}", self.at(f, "a", self.zk(k), pl.ds(0, 4)))

    def slot(self, name):
        for kind, *rest in STEPS[name]:
            getattr(self, kind)(*rest)


def layer_kernel(
    q_hbm,
    k_hbm,
    v_hbm,
    og_hbm,
    ig_hbm,
    fg_hbm,
    hg_hbm,
    wo_hbm,
    st_hbm,
    gain_hbm,
    wg_hbm,
    wu_hbm,
    wd_hbm,
    o_ref,
    ua,
    ub,
    da,
    db,
    q_ref,
    k_ref,
    v_ref,
    og_ref,
    ig_ref,
    fg_ref,
    hg_ref,
    wo,
    st_ref,
    gain_ref,
    acc,
    hid,
    y_ref,
    small1,
    small2,
    small_l,
    small_me,
    small_t,
    s_loc,
    r1,
    pre_l,
    t_loc,
    r2,
    o3,
    r3,
    part,
    rpart,
    sq_me,
    rsq,
    yloc,
    part2,
    rpart2,
    lsem,
    ss,
    rs,
    wss,
    wrs,
):
    sp, tp = lax.axis_index("sp"), lax.axis_index("tp")
    z, g = sp // NG, lax.rem(sp, NG)
    gpeer = [lax.rem(g + r, NG) for r in range(NG)]
    gfrom = [lax.rem(g + NG - r, NG) for r in range(NG)]
    zpeer = [lax.rem(z + r, NZ) for r in range(NZ)]
    xpeer = [lax.rem(tp + r, NX) for r in range(NX)]
    xfrom = [lax.rem(tp + NX - r, NX) for r in range(NX)]
    gdev = [{"sp": z * NG + p, "tp": tp} for p in gpeer]
    zdev = [{"sp": p * NG + g, "tp": tp} for p in zpeer]
    xdev = [{"sp": sp, "tp": p} for p in xpeer]
    def joint(n, ref):
        return copy_to(ref, ref, ss.at[n], rs.at[n], gdev[1])

    bar, count = barrier_all(gdev[1:] + zdev[1:] + xdev[1:])
    bufs = {("u", "a"): ua, ("u", "b"): ub, ("d", "a"): da, ("d", "b"): db}
    net = Weights(bufs, wss, wrs, z, g, tp)
    loads = []
    for f, kind, ref in (("u", 0, wg_hbm), ("u", 1, wu_hbm), ("d", 0, wd_hbm)):
        cut = SPLIT[f]
        for route, lanes in (("a", pl.ds(0, cut)), ("b", pl.ds(cut, FFT - cut))):
            loads.append(
                pltpu.make_async_copy(
                    ref.at[:, lanes], bufs[f, route].at[kind, z, net.c, net.y], lsem.at[len(loads)]
                )
            )
    early = ((fg_hbm, fg_ref), (ig_hbm, ig_ref), (k_hbm, k_ref), (v_hbm, v_ref), (q_hbm, q_ref))
    late = ((wo_hbm, wo), (og_hbm, og_ref), (hg_hbm, hg_ref), (st_hbm, st_ref), (gain_hbm, gain_ref))
    for src, dst in early + late:
        loads.append(pltpu.make_async_copy(src, dst, lsem.at[len(loads)]))
    for c in loads:
        c.start()
    for c in loads[:6]:
        c.wait()
    pl.semaphore_wait(bar, count)
    net.slot("first")
    for c in loads[6:11]:
        c.wait()
    rows = lax.broadcasted_iota(jnp.int32, (TOK, TOK), 0)
    cols = lax.broadcasted_iota(jnp.int32, (TOK, TOK), 1)
    eye = rows == cols
    low = rows >= cols

    lf = log_sigmoid(fg_ref[...])
    ig = ig_ref[...]
    small_me[...] = jnp.zeros_like(small_me)
    cs_cols, pairs, wks = [], [], []
    for h in range(2):
        lf_row = lf[h : h + 1, :]
        lf_col = col_of(lf_row, eye)
        cs_col = jnp.sum(jnp.where(low, lf_row, 0.0), axis=1, keepdims=True)
        cs_row = jnp.sum(jnp.where(rows <= cols, lf_col, 0.0), axis=0, keepdims=True)
        ig_row = ig[h : h + 1, :]
        rest_row = ig_row - cs_row
        rest_col = col_of(rest_row, eye)
        top = jnp.max(rest_row, axis=1, keepdims=True)
        total = jnp.sum(lf_row, axis=1, keepdims=True)
        wk = jnp.exp(rest_col - top) * k_ref[:, h * DQK : (h + 1) * DQK].astype(f32)
        small_me[h : h + 1, :] = jnp.sum(wk, axis=0, keepdims=True)
        small_me[2 + h : 3 + h, :] = jnp.broadcast_to(total, (1, TOK))
        small_me[4 + h : 5 + h, :] = jnp.broadcast_to(total + top, (1, TOK))
        cs_cols.append(cs_col)
        pairs.append((rest_row, ig_row))
        wks.append(wk)
    for h in range(2):
        hi, lo = split_hi_lo(wks[h])
        v_h = v_ref[:, h * DV : (h + 1) * DV]
        state = dot(hi, v_h, ((0,), (0,))) + dot(lo, v_h, ((0,), (0,)))
        s_loc[4 * h : 4 * h + 4] = state.astype(bf16).reshape(4, 32, DV)
    scale = DQK**-0.5
    num0, den0, peak0 = [], [], []
    for h in range(2):
        rest_row, ig_row = pairs[h]
        q_h = q_ref[:, h * DQK : (h + 1) * DQK]
        k_h = k_ref[:, h * DQK : (h + 1) * DQK]
        log_pair = jnp.where(low, cs_cols[h] + rest_row, -jnp.inf)
        peak = jnp.max(log_pair, axis=1, keepdims=True)
        scores = dot(q_h, k_h, ((1,), (1,))) * scale * jnp.exp(log_pair - peak)
        hi, lo = split_hi_lo(scores)
        v_h = v_ref[:, h * DV : (h + 1) * DV]
        num0.append(dot(hi, v_h) + dot(lo, v_h))
        den0.append(jnp.sum(scores, axis=1, keepdims=True))
        peak0.append(peak)

    net.slot("gates")
    for r in range(1, NG):
        copy_to(small_me, small1.at[g], ss.at[0], rs.at[0], gdev[r]).start()
        copy_to(s_loc.at[gpeer[r]], r1.at[g], ss.at[1], rs.at[1], gdev[r]).start()
    small1[g] = small_me[...]
    r1[g] = s_loc[g]
    net.slot("slices")
    joint(0, small1.at[pl.ds(0, NG - 1)]).wait_recv()
    n_l = jnp.zeros((2, TOK), f32)
    a_l = jnp.zeros((2, TOK), f32)
    m_l = jnp.full((2, TOK), very_low, f32)
    a_list, m_list, f_list, l_list = [], [], [], []
    for i in range(NG):
        small_l[i, 0:2, :] = n_l
        small_l[i, 2:4, :] = a_l
        small_l[i, 4:6, :] = m_l
        a_list.append(a_l)
        m_list.append(m_l)
        n_i, a_i, m_i = small1[i, 0:2, :], small1[i, 2:4, :], small1[i, 4:6, :]
        new = jnp.maximum(a_i + m_l, m_i)
        former, latter = jnp.exp(a_i + m_l - new), jnp.exp(m_i - new)
        f_list.append(former)
        l_list.append(latter)
        n_l = former * n_l + latter * n_i
        a_l = a_l + a_i
        m_l = new
    small_t[...] = jnp.zeros_like(small_t)
    small_t[0:2, :] = n_l
    small_t[2:4, :] = a_l
    small_t[4:6, :] = m_l
    for r in range(1, NZ):
        copy_to(small_t, small2.at[z], ss.at[2], rs.at[2], zdev[r]).start()
    small2[z] = small_t[...]

    def mine(pair):
        return jnp.where(g < 4, pair[0:1, :], pair[1:2, :])

    def spread(line):
        return jnp.concatenate([line, line], axis=1)

    joint(1, r1.at[pl.ds(0, NG - 1)]).wait_recv()
    run = jnp.zeros((32, DV), f32)
    for i in range(NG):
        pre_l[i] = run
        run = spread(mine(f_list[i])) * run + spread(mine(l_list[i])) * r1[i].astype(f32)
    t_loc[...] = run.astype(bf16)
    for r in range(1, NZ):
        copy_to(t_loc, r2.at[z], ss.at[3], rs.at[3], zdev[r]).start()
    r2[z] = t_loc[...]
    net.slot("totals")

    joint(2, small2.at[pl.ds(0, NZ - 1)]).wait_recv()
    n_z = jnp.zeros((2, TOK), f32)
    m_z = jnp.full((2, TOK), very_low, f32)
    fz, lz = [], []
    for i in range(NZ):
        on = i < z
        n_i, a_i, m_i = small2[i, 0:2, :], small2[i, 2:4, :], small2[i, 4:6, :]
        new = jnp.maximum(a_i + m_z, m_i)
        former, latter = jnp.exp(a_i + m_z - new), jnp.exp(m_i - new)
        former = jnp.where(on, former, 1.0)
        latter = jnp.where(on, latter, 0.0)
        fz.append(mine(former))
        lz.append(mine(latter))
        n_z = former * n_z + latter * n_i
        m_z = jnp.where(on, new, m_z)
    ca, cb = [], []
    for j in range(NG):
        new = jnp.maximum(a_list[j] + m_z, m_list[j])
        ca.append(mine(jnp.exp(m_list[j] - new)))
        cb.append(mine(jnp.exp(a_list[j] + m_z - new)))
    n_g, a_g, m_g = small_l[g, 0:2, :], small_l[g, 2:4, :], small_l[g, 4:6, :]
    m_in = jnp.maximum(a_g + m_z, m_g)
    n_in = jnp.exp(m_g - m_in) * n_g + jnp.exp(a_g + m_z - m_in) * n_z

    scale0, carried, denom = [], [], []
    for h in range(2):
        q_h = q_ref[:, h * DQK : (h + 1) * DQK].astype(f32)
        log_carry = cs_cols[h] + m_in[h : h + 1, 0:1]
        peak = jnp.maximum(peak0[h], log_carry)
        s0, c0 = jnp.exp(peak0[h] - peak), jnp.exp(log_carry - peak) * scale
        normer = s0 * den0[h] + c0 * jnp.sum(q_h * n_in[h : h + 1, :], axis=1, keepdims=True)
        inv = 1.0 / jnp.maximum(jnp.abs(normer), jnp.exp(-peak))
        scale0.append(s0 * inv)
        carried.append(c0 * inv)

    joint(3, r2.at[pl.ds(0, NZ - 1)]).wait_recv()
    run = jnp.zeros((32, DV), f32)
    for i in range(NZ):
        run = spread(fz[i]) * run + spread(lz[i]) * r2[i].astype(f32)
    for j in range(NG):
        o3[j] = (spread(ca[j]) * pre_l[j] + spread(cb[j]) * run).astype(bf16)
    for r in range(1, NG):
        copy_to(o3.at[gpeer[r]], r3.at[g], ss.at[4], rs.at[4], gdev[r]).start()
    r3[g] = o3[g]
    net.slot("prefix")
    for c in loads[11:]:
        c.wait()
    gates = [
        hg_ref[:, h * DV : (h + 1) * DV]
        / (1.0 + jnp.exp(-og_ref[:, h * DV : (h + 1) * DV].astype(f32)))
        for h in range(2)
    ]
    joint(4, r3.at[pl.ds(0, NG - 1)]).wait_recv()
    gated, sq = [], jnp.zeros((TOK, 1), f32)
    for h in range(2):
        q_h = q_ref[:, h * DQK : (h + 1) * DQK]
        state = r3[4 * h : 4 * h + 4].reshape(DQK, DV)
        out = scale0[h] * num0[h] + carried[h] * dot(q_h, state)
        sq = sq + jnp.sum(out * out, axis=1, keepdims=True)
        gated.append((out * gates[h]).astype(bf16))
    sq_me[0] = jnp.broadcast_to(row_of(sq, eye), (8, TOK))
    for r in range(1, NX):
        copy_to(sq_me.at[0], rsq.at[0, tp], ss.at[5], rs.at[5], xdev[r]).start()
    rsq[0, tp] = sq_me[0]
    heads = jnp.concatenate(gated, axis=1)
    for r in (2, 1, 3, 0):
        at = pl.multiple_of(xpeer[r] * COLS, COLS)
        part[xpeer[r]] = dot(heads, wo[:, pl.ds(at, COLS)]).astype(bf16)
        if r:
            copy_to(part.at[xpeer[r]], rpart.at[tp], ss.at[6], rs.at[6], xdev[r]).start()
    rpart[tp] = part[tp]
    net.slot("parts")
    joint(5, rsq.at[0, pl.ds(0, NX - 1)]).wait_recv()
    sq_all = jnp.sum(rsq[0, :, 0, :], axis=0, keepdims=True)
    row_scale = col_of(lax.rsqrt(sq_all / VALS + norm_eps), eye)
    joint(6, rpart.at[pl.ds(0, NX - 1)]).wait_recv()
    mixer = rpart[0].astype(f32)
    for i in range(1, NX):
        mixer = mixer + rpart[i].astype(f32)
    resid = (st_ref[...].astype(f32) + mixer * row_scale).astype(bf16)
    resid_f = resid.astype(f32)
    gain = gain_ref[:, pl.ds(pl.multiple_of(tp * COLS, COLS), COLS)]
    yloc[...] = (resid_f * gain).astype(bf16)
    sq_me[1] = jnp.broadcast_to(
        row_of(jnp.sum(resid_f * resid_f, axis=1, keepdims=True), eye), (8, TOK)
    )
    for r in (2, 1, 3):
        copy_to(yloc, y_ref.at[tp], ss.at[8], rs.at[8], xdev[r]).start()
    for r in range(1, NX):
        copy_to(sq_me.at[1], rsq.at[1, tp], ss.at[7], rs.at[7], xdev[r]).start()
    rsq[1, tp] = sq_me[1]
    y_ref[tp] = yloc[...]
    net.slot("feats")
    joint(7, rsq.at[1, pl.ds(0, NX - 1)]).wait_recv()
    sq_all = jnp.sum(rsq[1, :, 0, :], axis=0, keepdims=True)
    scale_in = col_of(lax.rsqrt(sq_all / D + norm_eps), eye)
    joint(8, y_ref.at[pl.ds(0, NX - 1)]).wait_recv()
    def y_col(zi):
        return y_ref[zi // 2, :, pl.ds(pl.multiple_of(lax.rem(zi, 2) * 256, 256), 256)]

    seen = set()

    def rows_of(f, route, kind, zi):
        buf = bufs[f, route]
        return [buf[kind, zi, core, yi] for yi in range(4) for core in range(2)]

    def column(route, zi):
        cut = SPLIT["u"]
        lanes = pl.ds(0, cut) if route == "a" else pl.ds(cut, FFT - cut)
        for kind in range(2):
            term = dot(y_col(zi), jnp.concatenate(rows_of("u", route, kind, zi), axis=0))
            if (route, kind) in seen:
                acc[kind, :, lanes] += term
            else:
                acc[kind, :, lanes] = term
            seen.add((route, kind))

    for kind, *rest in STEPS["rest"]:
        if kind == "fb":
            net.column_b(*rest)
            column("b", net.zi[rest[1]])
        elif kind == "fa":
            net.column_a(*rest)
            column("a", net.zk(rest[1]))
        elif kind == "hid":
            gate = acc[0] * scale_in
            hid[...] = (gate / (1.0 + jnp.exp(-gate)) * (acc[1] * scale_in)).astype(bf16)
        elif kind == "dn":
            net.column_b("d", COLUMNS.index(rest[1]))
            net.column_a("d", rest[1])
            zi = net.zk(rest[1])
            at = zi // 2
            cut = SPLIT["d"]
            term = jnp.zeros((TOK, 256), f32)
            for route, lanes in (("a", pl.ds(0, cut)), ("b", pl.ds(cut, FFT - cut))):
                rows_d = jnp.concatenate(rows_of("d", route, 0, zi), axis=0)
                term = term + dot(hid[:, lanes], rows_d, ((1,), (1,)))
            part2[zi] = term.astype(bf16)

            @pl.when(at != tp)
            def _():
                copy_to(
                    part2.at[zi],
                    rpart2.at[tp, lax.rem(zi, 2)],
                    ss.at[9],
                    rs.at[9],
                    {"sp": sp, "tp": at},
                ).start()
        else:
            getattr(net, kind)(*rest)
    joint(9, rpart2.at[pl.ds(0, NX - 1)]).wait_recv()
    for half in range(2):
        lanes = slice(256 * half, 256 * half + 256)
        total = resid_f[:, lanes] + part2[2 * tp + half].astype(f32)
        for r in range(1, NX):
            total = total + rpart2[xfrom[r], half].astype(f32)
        o_ref[:, lanes] = total.astype(bf16)
    for n, ref in enumerate(
        (
            small1.at[pl.ds(0, NG - 1)],
            r1.at[pl.ds(0, NG - 1)],
            small2.at[pl.ds(0, NZ - 1)],
            r2.at[pl.ds(0, NZ - 1)],
            r3.at[pl.ds(0, NG - 1)],
            rsq.at[0, pl.ds(0, NX - 1)],
            rpart.at[pl.ds(0, NX - 1)],
            rsq.at[1, pl.ds(0, NX - 1)],
            y_ref.at[pl.ds(0, NX - 1)],
            rpart2.at[pl.ds(0, NX - 1)],
        )
    ):
        joint(n, ref).wait_send()
    net.drain()


def local(
    stream,
    queries,
    keys,
    values,
    out_gate,
    input_gate,
    forget_gate,
    head_gain,
    w_out,
    ffn_gain,
    w_gate,
    w_up,
    w_down,
):
    vmem = pl.BlockSpec(memory_space=pltpu.VMEM)
    hbm = pl.BlockSpec(memory_space=pl.ANY)
    return pl.pallas_call(
        layer_kernel,
        out_shape=pltpu.VMEM((TOK, COLS), bf16),
        in_specs=[hbm] * 13,
        out_specs=vmem,
        scratch_shapes=[
            pltpu.VMEM((2, NZ, 2, 4, 32, SPLIT["u"]), bf16),
            pltpu.VMEM((2, NZ, 2, 4, 32, FFT - SPLIT["u"]), bf16),
            pltpu.VMEM((1, NZ, 2, 4, 32, SPLIT["d"]), bf16),
            pltpu.VMEM((1, NZ, 2, 4, 32, FFT - SPLIT["d"]), bf16),
            pltpu.VMEM((TOK, 2 * DQK), bf16),
            pltpu.VMEM((TOK, 2 * DQK), bf16),
            pltpu.VMEM((TOK, COLS), bf16),
            pltpu.VMEM((TOK, COLS), bf16),
            pltpu.VMEM((2, TOK), f32),
            pltpu.VMEM((2, TOK), f32),
            pltpu.VMEM((1, COLS), f32),
            pltpu.VMEM((COLS, D), bf16),
            pltpu.VMEM((TOK, COLS), bf16),
            pltpu.VMEM((1, D), f32),
            pltpu.VMEM((2, TOK, FFT), f32),
            pltpu.VMEM((TOK, FFT), bf16),
            pltpu.VMEM((NX, TOK, COLS), bf16),
            pltpu.VMEM((NG, 8, TOK), f32),
            pltpu.VMEM((NZ, 8, TOK), f32),
            pltpu.VMEM((NG, 8, TOK), f32),
            pltpu.VMEM((8, TOK), f32),
            pltpu.VMEM((8, TOK), f32),
            pltpu.VMEM((NG, 32, DV), bf16),
            pltpu.VMEM((NG, 32, DV), bf16),
            pltpu.VMEM((NG, 32, DV), f32),
            pltpu.VMEM((32, DV), bf16),
            pltpu.VMEM((NZ, 32, DV), bf16),
            pltpu.VMEM((NG, 32, DV), bf16),
            pltpu.VMEM((NG, 32, DV), bf16),
            pltpu.VMEM((NX, TOK, COLS), bf16),
            pltpu.VMEM((NX, TOK, COLS), bf16),
            pltpu.VMEM((2, 8, TOK), f32),
            pltpu.VMEM((2, NX, 8, TOK), f32),
            pltpu.VMEM((TOK, COLS), bf16),
            pltpu.VMEM((NZ, TOK, 256), bf16),
            pltpu.VMEM((NX, 2, TOK, 256), bf16),
            pltpu.SemaphoreType.DMA((16,)),
            pltpu.SemaphoreType.DMA((10,)),
            pltpu.SemaphoreType.DMA((10,)),
            pltpu.SemaphoreType.DMA((5 * RING,)),
            pltpu.SemaphoreType.DMA((84,)),
        ],
        compiler_params=pltpu.CompilerParams(
            collective_id=0, has_side_effects=True, vmem_limit_bytes=60 * 2**20
        ),
    )(
        queries,
        keys,
        values,
        out_gate,
        input_gate.T,
        forget_gate.T,
        head_gain.reshape(1, COLS),
        w_out,
        stream,
        ffn_gain.reshape(1, D),
        w_gate,
        w_up,
        w_down.T,
    )


def solution(mesh):
    in_specs = (
        P("sp", "tp"),
        P("sp", "tp"),
        P("sp", "tp"),
        P("sp", "tp"),
        P("sp", "tp"),
        P("sp", "tp"),
        P("sp", "tp"),
        P("tp"),
        P("tp", None),
        P(),
        P("sp", "tp"),
        P("sp", "tp"),
        P("tp", "sp"),
    )
    return jax.shard_map(
        local, mesh=mesh, in_specs=in_specs, out_specs=P("sp", "tp"), check_vma=False
    )
```

```python
import functools

import jax
import jax.numpy as jnp
from jax import lax
from jax.experimental import pallas as pl
from jax.experimental.pallas import tpu as pltpu
from jax.sharding import PartitionSpec as P

D = 2048
DQK = 128
DV = 256
VALS = 2048
FFT = 1408
TOK = 128
COLS = 512
NG = 8
NZ = 8
NX = 4
norm_eps = 1e-06
very_low = -1e30
MESH = pl.DeviceIdType.MESH
f32 = jnp.float32
bf16 = jnp.bfloat16


def row_of(col, eye):
    return jnp.sum(jnp.where(eye, col, 0.0), axis=0, keepdims=True)


def col_of(row, eye):
    return jnp.sum(jnp.where(eye, row, 0.0), axis=1, keepdims=True)


def split_hi_lo(x):
    hi = x.astype(bf16)
    return hi, (x - hi.astype(f32)).astype(bf16)


def dot(a, b, dims=((1,), (0,))):
    return lax.dot_general(a, b, (dims, ((), ())), preferred_element_type=f32)


def log_sigmoid(x):
    return jnp.minimum(x, 0.0) - jnp.log1p(jnp.exp(-jnp.abs(x)))


def copy_to(src, dst, ssem, rsem, dev):
    return pltpu.make_async_remote_copy(
        src_ref=src, dst_ref=dst, send_sem=ssem, recv_sem=rsem, device_id=dev, device_id_type=MESH
    )


def barrier_all(devs):
    bar = pltpu.get_barrier_semaphore()
    for dev in devs:
        pl.semaphore_signal(bar, inc=1, device_id=dev, device_id_type=MESH)
    return bar, len(devs)


RING = 6
COLUMNS = (0, -1, 1, -2, 2, -3, 3, 4)
SPLIT = {"u": 512, "d": 640}
STEPS = {
    "first": (
        ("own", "d"),
    ),
    "gates": (
    ),
    "slices": (
        ("own", "u"),
        ("by", "u", 0),
        ("bz", "d", 1),
        ("by", "d", 0),
    ),
    "totals": (
        ("ayf", "u"),
        ("bz", "u", 1),
        ("by", "u", 2),
        ("az", "u", 0),
        ("by", "u", 1),
        ("by", "d", 1),
    ),
    "prefix": (
        ("bz", "u", 2),
        ("byf", "u", 0),
        ("sa", "u", 0),
        ("by", "u", 3),
        ("by", "d", 2),
        ("bz", "d", 2),
        ("byf", "u", 1),
        ("ayf", "d"),
        ("az", "u", 1),
        ("bz", "u", 3),
        ("by", "u", 5),
    ),
    "parts": (
        ("byf", "u", 2),
        ("byf", "u", 3),
        ("by", "u", 4),
        ("az", "d", 0),
        ("by", "u", 6),
        ("sb", "u", 1),
        ("bz", "u", 4),
        ("az", "u", 2),
        ("sb", "u", 2),
        ("sb", "u", 0),
        ("sa", "u", -1),
        ("by", "u", 7),
        ("sa", "d", 0),
    ),
    "feats": (
        ("sa", "u", 2),
        ("sa", "u", -2),
        ("sa", "u", 1),
        ("byf", "u", 5),
        ("byf", "u", 4),
        ("byf", "d", 0),
        ("byf", "u", 6),
        ("sb", "u", 3),
        ("az", "d", 1),
        ("byf", "u", 7),
        ("sb", "u", 5),
        ("az", "u", 3),
        ("byf", "d", 1),
        ("byf", "d", 2),
        ("sb", "u", 4),
        ("bz", "d", 3),
        ("sb", "d", 0),
    ),
    "rest": (
        ("by", "d", 4),
        ("sa", "d", -1),
        ("fb", "u", 2),
        ("fb", "u", 1),
        ("fb", "u", 0),
        ("by", "d", 3),
        ("sa", "u", -3),
        ("fa", "u", 1),
        ("fb", "u", 5),
        ("by", "d", 5),
        ("sb", "u", 7),
        ("az", "d", 2),
        ("sb", "u", 6),
        ("sa", "u", 3),
        ("by", "d", 6),
        ("fb", "u", 4),
        ("fa", "u", -2),
        ("fa", "u", 2),
        ("az", "u", 4),
        ("sa", "u", 4),
        ("byf", "d", 4),
        ("fa", "u", -3),
        ("byf", "d", 3),
        ("fb", "u", 7),
        ("bz", "d", 4),
        ("by", "d", 7),
        ("sb", "d", 1),
        ("fb", "u", 6),
        ("sa", "d", -2),
        ("fa", "u", -1),
        ("fa", "u", 3),
        ("sb", "d", 2),
        ("fa", "u", 0),
        ("sa", "d", 2),
        ("fb", "u", 3),
        ("sa", "d", 1),
        ("fa", "u", 4),
        ("byf", "d", 5),
        ("hid", "u"),
        ("dn", "d", 0),
        ("dn", "d", -1),
        ("byf", "d", 6),
        ("sb", "d", 3),
        ("sb", "d", 4),
        ("az", "d", 3),
        ("sa", "d", -3),
        ("byf", "d", 7),
        ("dn", "d", 1),
        ("sb", "d", 5),
        ("dn", "d", -2),
        ("sb", "d", 6),
        ("sa", "d", 3),
        ("dn", "d", 2),
        ("dn", "d", -3),
        ("sb", "d", 7),
        ("az", "d", 4),
        ("sa", "d", 4),
        ("dn", "d", 3),
        ("dn", "d", 4),
    ),
}


class Weights:
    def __init__(self, bufs, ssem, rsem, z, g, tp):
        self.bufs, self.ssem, self.rsem = bufs, ssem, rsem
        self.z, self.y, self.c, self.tp = z, g // 2, lax.rem(g, 2), tp
        self.ids, self.sent = {}, {}
        self.zi = [self.zk(k) for k in COLUMNS]

        def z_at(k):
            return {"sp": lax.rem(z + k, NZ) * NG + g, "tp": tp}

        def y_at(k):
            return {"sp": z * NG + lax.rem(self.y + k, 4) * 2 + self.c, "tp": tp}

        self.dev = {
            "z+": z_at(1),
            "z-": z_at(7),
            "y+": y_at(1),
            "y-": y_at(3),
            "s": {"sp": z * NG + self.y * 2 + (1 - self.c), "tp": tp},
        }
        self.ways = list(self.dev)

    def zk(self, k):
        return lax.rem(self.z + NZ + k, NZ)

    def yk(self, k):
        return lax.rem(self.y + 4 + k, 4)

    def at(self, f, route, zi, yi, half=None, core=None):
        kinds, rows = pl.ds(0, 2 if f == "u" else 1), pl.ds(0, 32)
        if half is not None:
            kinds, rows = (pl.ds(half, 1), rows) if f == "u" else (kinds, pl.ds(16 * half, 16))
        zs = zi if isinstance(zi, pl.Slice) else pl.ds(zi, 1)
        ys = yi if isinstance(yi, pl.Slice) else pl.ds(yi, 1)
        return self.bufs[f, route].at[kinds, zs, self.c if core is None else core, ys, rows]

    def send(self, name, way, ref):
        n = self.ids.setdefault(name, len(self.ids))
        past = self.sent.setdefault(way, [])
        k = len(past)
        if k >= RING:
            past[k - RING].wait_send()
        slot = self.ways.index(way) * RING + k % RING
        c = copy_to(ref, ref, self.ssem.at[slot], self.rsem.at[n], self.dev[way])
        c.start()
        past.append(c)

    def got(self, name, ref):
        n = self.ids.setdefault(name, len(self.ids))
        copy_to(ref, ref, self.ssem.at[0], self.rsem.at[n], self.dev["s"]).wait_recv()

    def drain(self):
        for past in self.sent.values():
            for c in past[-RING:]:
                c.wait_send()

    def own(self, f):
        for way in ("z+", "z-"):
            self.send(f"bz{f}1", way, self.at(f, "b", self.z, self.y))
        for way in ("y+", "y-"):
            self.send(f"ay{f}", way, self.at(f, "a", self.z, self.y))

    def bz(self, f, k):
        self.got(f"bz{f}{k}", self.at(f, "b", pl.ds(0, 1 if k == 4 else 2), self.y))
        if k < 4:
            halves = (0, 1) if k == 3 else (None, None)
            self.send(f"bz{f}{k + 1}", "z+", self.at(f, "b", self.zk(-k), self.y, halves[0]))
            self.send(f"bz{f}{k + 1}", "z-", self.at(f, "b", self.zk(k), self.y, halves[1]))

    def by(self, f, j):
        for way in ("y+", "y-"):
            self.send(f"by{f}{j}", way, self.at(f, "b", self.zi[j], self.y))

    def byf(self, f, j):
        self.got(f"by{f}{j}", self.at(f, "b", self.zi[j], pl.ds(0, 2)))
        self.send(f"byf{f}{j}", "y+", self.at(f, "b", self.zi[j], self.yk(-1), 0))
        self.send(f"byf{f}{j}", "y-", self.at(f, "b", self.zi[j], self.yk(1), 1))

    def sb(self, f, j):
        self.got(f"byf{f}{j}", self.at(f, "b", self.zi[j], self.yk(2)))
        self.send(f"sb{f}{j}", "s", self.at(f, "b", self.zi[j], pl.ds(0, 4)))

    def ayf(self, f):
        self.got(f"ay{f}", self.at(f, "a", self.z, pl.ds(0, 2)))
        self.send(f"ayf{f}", "y+", self.at(f, "a", self.z, self.yk(-1), 0))
        self.send(f"ayf{f}", "y-", self.at(f, "a", self.z, self.yk(1), 1))

    def sa(self, f, k):
        self.send(f"sa{f}{k}", "s", self.at(f, "a", self.zk(k), pl.ds(0, 4)))

    def az(self, f, k):
        if k == 0:
            self.got(f"ayf{f}", self.at(f, "a", self.z, self.yk(2)))
        else:
            self.got(f"az{f}{k}", self.at(f, "a", pl.ds(0, 1 if k == 4 else 2), pl.ds(0, 4)))
        if k == 4:
            return
        for p in range(2):
            for way, zi, mine in (("z+", self.zk(-k), 0), ("z-", self.zk(k), 1)):
                if k < 3 or p == mine:
                    self.send(f"az{f}{k + 1}", way, self.at(f, "a", zi, pl.ds(2 * p, 2)))

    def column_b(self, f, j):
        self.got(f"sb{f}{j}", self.at(f, "b", self.zi[j], pl.ds(0, 4)))

    def column_a(self, f, k):
        self.got(f"sa{f}{k}", self.at(f, "a", self.zk(k), pl.ds(0, 4)))

    def slot(self, name):
        for kind, *rest in STEPS[name]:
            getattr(self, kind)(*rest)


def layer_kernel(
    q_hbm,
    k_hbm,
    v_hbm,
    og_hbm,
    ig_hbm,
    fg_hbm,
    hg_hbm,
    wo_hbm,
    st_hbm,
    gain_hbm,
    wg_hbm,
    wu_hbm,
    wd_hbm,
    o_ref,
    ua,
    ub,
    da,
    db,
    q_ref,
    k_ref,
    v_ref,
    og_ref,
    ig_ref,
    fg_ref,
    hg_ref,
    wo,
    st_ref,
    gain_ref,
    acc,
    hid,
    y_ref,
    small1,
    small2,
    small_l,
    small_me,
    small_t,
    s_loc,
    r1,
    pre_l,
    t_loc,
    r2,
    o3,
    r3,
    part,
    rpart,
    sq_me,
    rsq,
    yloc,
    part2,
    rpart2,
    lsem,
    ss,
    rs,
    wss,
    wrs,
):
    sp, tp = lax.axis_index("sp"), lax.axis_index("tp")
    z, g = sp // NG, lax.rem(sp, NG)
    gpeer = [lax.rem(g + r, NG) for r in range(NG)]
    gfrom = [lax.rem(g + NG - r, NG) for r in range(NG)]
    zpeer = [lax.rem(z + r, NZ) for r in range(NZ)]
    xpeer = [lax.rem(tp + r, NX) for r in range(NX)]
    xfrom = [lax.rem(tp + NX - r, NX) for r in range(NX)]
    gdev = [{"sp": z * NG + p, "tp": tp} for p in gpeer]
    zdev = [{"sp": p * NG + g, "tp": tp} for p in zpeer]
    xdev = [{"sp": sp, "tp": p} for p in xpeer]
    def joint(n, ref):
        return copy_to(ref, ref, ss.at[n], rs.at[n], gdev[1])

    r2[...] = jnp.zeros_like(r2)
    bar, count = barrier_all(gdev[1:] + zdev[1:] + xdev[1:])
    bufs = {("u", "a"): ua, ("u", "b"): ub, ("d", "a"): da, ("d", "b"): db}
    net = Weights(bufs, wss, wrs, z, g, tp)
    loads = []
    for f, kind, ref in (("u", 0, wg_hbm), ("u", 1, wu_hbm), ("d", 0, wd_hbm)):
        cut = SPLIT[f]
        for route, lanes in (("a", pl.ds(0, cut)), ("b", pl.ds(cut, FFT - cut))):
            loads.append(
                pltpu.make_async_copy(
                    ref.at[:, lanes], bufs[f, route].at[kind, z, net.c, net.y], lsem.at[len(loads)]
                )
            )
    early = ((fg_hbm, fg_ref), (ig_hbm, ig_ref), (k_hbm, k_ref), (v_hbm, v_ref), (q_hbm, q_ref))
    late = ((wo_hbm, wo), (og_hbm, og_ref), (hg_hbm, hg_ref), (st_hbm, st_ref), (gain_hbm, gain_ref))
    for src, dst in early + late:
        loads.append(pltpu.make_async_copy(src, dst, lsem.at[len(loads)]))
    for c in loads:
        c.start()
    for c in loads[:6]:
        c.wait()
    for c in loads[6:11]:
        c.wait()
    rows = lax.broadcasted_iota(jnp.int32, (TOK, TOK), 0)
    cols = lax.broadcasted_iota(jnp.int32, (TOK, TOK), 1)
    eye = rows == cols
    low = rows >= cols

    lf = log_sigmoid(fg_ref[...])
    ig = ig_ref[...]
    small_me[...] = jnp.zeros_like(small_me)
    cs_cols, pairs, wks = [], [], []
    for h in range(2):
        lf_row = lf[h : h + 1, :]
        lf_col = col_of(lf_row, eye)
        cs_col = jnp.sum(jnp.where(low, lf_row, 0.0), axis=1, keepdims=True)
        cs_row = jnp.sum(jnp.where(rows <= cols, lf_col, 0.0), axis=0, keepdims=True)
        ig_row = ig[h : h + 1, :]
        rest_row = ig_row - cs_row
        rest_col = col_of(rest_row, eye)
        top = jnp.max(rest_row, axis=1, keepdims=True)
        total = jnp.sum(lf_row, axis=1, keepdims=True)
        wk = jnp.exp(rest_col - top) * k_ref[:, h * DQK : (h + 1) * DQK].astype(f32)
        small_me[h : h + 1, :] = jnp.sum(wk, axis=0, keepdims=True)
        small_me[2 + h : 3 + h, :] = jnp.broadcast_to(total, (1, TOK))
        small_me[4 + h : 5 + h, :] = jnp.broadcast_to(total + top, (1, TOK))
        cs_cols.append(cs_col)
        pairs.append((rest_row, ig_row))
        wks.append(wk)
    for h in range(2):
        hi, lo = split_hi_lo(wks[h])
        v_h = v_ref[:, h * DV : (h + 1) * DV]
        state = dot(hi, v_h, ((0,), (0,))) + dot(lo, v_h, ((0,), (0,)))
        s_loc[4 * h : 4 * h + 4] = state.astype(bf16).reshape(4, 32, DV)
    scale = DQK**-0.5
    num0, den0, peak0 = [], [], []
    for h in range(2):
        rest_row, ig_row = pairs[h]
        q_h = q_ref[:, h * DQK : (h + 1) * DQK]
        k_h = k_ref[:, h * DQK : (h + 1) * DQK]
        log_pair = jnp.where(low, cs_cols[h] + rest_row, -jnp.inf)
        peak = jnp.max(log_pair, axis=1, keepdims=True)
        scores = dot(q_h, k_h, ((1,), (1,))) * scale * jnp.exp(log_pair - peak)
        hi, lo = split_hi_lo(scores)
        v_h = v_ref[:, h * DV : (h + 1) * DV]
        num0.append(dot(hi, v_h) + dot(lo, v_h))
        den0.append(jnp.sum(scores, axis=1, keepdims=True))
        peak0.append(peak)

    pl.semaphore_wait(bar, count)
    net.slot("first")
    net.slot("gates")
    for r in range(1, NG):
        copy_to(small_me, small1.at[g], ss.at[0], rs.at[0], gdev[r]).start()
        copy_to(s_loc.at[gpeer[r]], r1.at[g], ss.at[1], rs.at[1], gdev[r]).start()
    small1[g] = small_me[...]
    r1[g] = s_loc[g]
    net.slot("slices")
    joint(0, small1.at[pl.ds(0, NG - 1)]).wait_recv()
    n_l = jnp.zeros((2, TOK), f32)
    a_l = jnp.zeros((2, TOK), f32)
    m_l = jnp.full((2, TOK), very_low, f32)
    a_list, m_list, f_list, l_list = [], [], [], []
    for i in range(NG):
        small_l[i, 0:2, :] = n_l
        small_l[i, 2:4, :] = a_l
        small_l[i, 4:6, :] = m_l
        a_list.append(a_l)
        m_list.append(m_l)
        n_i, a_i, m_i = small1[i, 0:2, :], small1[i, 2:4, :], small1[i, 4:6, :]
        new = jnp.maximum(a_i + m_l, m_i)
        former, latter = jnp.exp(a_i + m_l - new), jnp.exp(m_i - new)
        f_list.append(former)
        l_list.append(latter)
        n_l = former * n_l + latter * n_i
        a_l = a_l + a_i
        m_l = new
    small_t[...] = jnp.zeros_like(small_t)
    small_t[0:2, :] = n_l
    small_t[2:4, :] = a_l
    small_t[4:6, :] = m_l
    for r in range(1, NZ):
        copy_to(small_t, small2.at[z], ss.at[2], rs.at[2], zdev[r]).start()
    small2[z] = small_t[...]

    def mine(pair):
        return jnp.where(g < 4, pair[0:1, :], pair[1:2, :])

    def spread(line):
        return jnp.concatenate([line, line], axis=1)

    joint(1, r1.at[pl.ds(0, NG - 1)]).wait_recv()
    run = jnp.zeros((32, DV), f32)
    for i in range(NG):
        pre_l[i] = run
        run = spread(mine(f_list[i])) * run + spread(mine(l_list[i])) * r1[i].astype(f32)
    t_loc[...] = run.astype(bf16)
    for r in range(1, NZ):

        @pl.when(z + r < NZ)
        def _(r=r):
            copy_to(t_loc, r2.at[z], ss.at[10 + r], rs.at[10 + r], zdev[r]).start()

    r2[z] = t_loc[...]
    net.slot("totals")

    joint(2, small2.at[pl.ds(0, NZ - 1)]).wait_recv()
    n_z = jnp.zeros((2, TOK), f32)
    m_z = jnp.full((2, TOK), very_low, f32)
    fz, lz = [], []
    for i in range(NZ):
        on = i < z
        n_i, a_i, m_i = small2[i, 0:2, :], small2[i, 2:4, :], small2[i, 4:6, :]
        new = jnp.maximum(a_i + m_z, m_i)
        former, latter = jnp.exp(a_i + m_z - new), jnp.exp(m_i - new)
        former = jnp.where(on, former, 1.0)
        latter = jnp.where(on, latter, 0.0)
        fz.append(mine(former))
        lz.append(mine(latter))
        n_z = former * n_z + latter * n_i
        m_z = jnp.where(on, new, m_z)
    ca, cb = [], []
    for j in range(NG):
        new = jnp.maximum(a_list[j] + m_z, m_list[j])
        ca.append(mine(jnp.exp(m_list[j] - new)))
        cb.append(mine(jnp.exp(a_list[j] + m_z - new)))
    n_g, a_g, m_g = small_l[g, 0:2, :], small_l[g, 2:4, :], small_l[g, 4:6, :]
    m_in = jnp.maximum(a_g + m_z, m_g)
    n_in = jnp.exp(m_g - m_in) * n_g + jnp.exp(a_g + m_z - m_in) * n_z

    scale0, carried, denom = [], [], []
    for h in range(2):
        q_h = q_ref[:, h * DQK : (h + 1) * DQK].astype(f32)
        log_carry = cs_cols[h] + m_in[h : h + 1, 0:1]
        peak = jnp.maximum(peak0[h], log_carry)
        s0, c0 = jnp.exp(peak0[h] - peak), jnp.exp(log_carry - peak) * scale
        normer = s0 * den0[h] + c0 * jnp.sum(q_h * n_in[h : h + 1, :], axis=1, keepdims=True)
        inv = 1.0 / jnp.maximum(jnp.abs(normer), jnp.exp(-peak))
        scale0.append(s0 * inv)
        carried.append(c0 * inv)

    for r in range(1, NZ):

        @pl.when(z >= r)
        def _(r=r):
            joint(10 + r, r2.at[0]).wait_recv()

    run = jnp.zeros((32, DV), f32)
    for i in range(NZ):
        run = spread(fz[i]) * run + spread(lz[i]) * r2[i].astype(f32)
    for j in range(NG):
        o3[j] = (spread(ca[j]) * pre_l[j] + spread(cb[j]) * run).astype(bf16)
    for r in range(1, NG):
        copy_to(o3.at[gpeer[r]], r3.at[g], ss.at[4], rs.at[4], gdev[r]).start()
    r3[g] = o3[g]
    net.slot("prefix")
    for c in loads[11:]:
        c.wait()
    gates = [
        hg_ref[:, h * DV : (h + 1) * DV]
        / (1.0 + jnp.exp(-og_ref[:, h * DV : (h + 1) * DV].astype(f32)))
        for h in range(2)
    ]
    joint(4, r3.at[pl.ds(0, NG - 1)]).wait_recv()
    gated, sq = [], jnp.zeros((TOK, 1), f32)
    for h in range(2):
        q_h = q_ref[:, h * DQK : (h + 1) * DQK]
        state = r3[4 * h : 4 * h + 4].reshape(DQK, DV)
        out = scale0[h] * num0[h] + carried[h] * dot(q_h, state)
        sq = sq + jnp.sum(out * out, axis=1, keepdims=True)
        gated.append((out * gates[h]).astype(bf16))
    sq_me[0] = jnp.broadcast_to(row_of(sq, eye), (8, TOK))
    for r in range(1, NX):
        copy_to(sq_me.at[0], rsq.at[0, tp], ss.at[5], rs.at[5], xdev[r]).start()
    rsq[0, tp] = sq_me[0]
    heads = jnp.concatenate(gated, axis=1)
    for r in (2, 1, 3, 0):
        at = pl.multiple_of(xpeer[r] * COLS, COLS)
        part[xpeer[r]] = dot(heads, wo[:, pl.ds(at, COLS)]).astype(bf16)
        if r:
            copy_to(part.at[xpeer[r]], rpart.at[tp], ss.at[6], rs.at[6], xdev[r]).start()
    rpart[tp] = part[tp]
    net.slot("parts")
    joint(5, rsq.at[0, pl.ds(0, NX - 1)]).wait_recv()
    sq_all = jnp.sum(rsq[0, :, 0, :], axis=0, keepdims=True)
    row_scale = col_of(lax.rsqrt(sq_all / VALS + norm_eps), eye)
    joint(6, rpart.at[pl.ds(0, NX - 1)]).wait_recv()
    mixer = rpart[0].astype(f32)
    for i in range(1, NX):
        mixer = mixer + rpart[i].astype(f32)
    resid = (st_ref[...].astype(f32) + mixer * row_scale).astype(bf16)
    resid_f = resid.astype(f32)
    gain = gain_ref[:, pl.ds(pl.multiple_of(tp * COLS, COLS), COLS)]
    yloc[...] = (resid_f * gain).astype(bf16)
    sq_me[1] = jnp.broadcast_to(
        row_of(jnp.sum(resid_f * resid_f, axis=1, keepdims=True), eye), (8, TOK)
    )
    for r in (2, 1, 3):
        copy_to(yloc, y_ref.at[tp], ss.at[8], rs.at[8], xdev[r]).start()
    for r in range(1, NX):
        copy_to(sq_me.at[1], rsq.at[1, tp], ss.at[7], rs.at[7], xdev[r]).start()
    rsq[1, tp] = sq_me[1]
    y_ref[tp] = yloc[...]
    net.slot("feats")
    joint(7, rsq.at[1, pl.ds(0, NX - 1)]).wait_recv()
    sq_all = jnp.sum(rsq[1, :, 0, :], axis=0, keepdims=True)
    scale_in = col_of(lax.rsqrt(sq_all / D + norm_eps), eye)
    joint(8, y_ref.at[pl.ds(0, NX - 1)]).wait_recv()
    def y_col(zi):
        return y_ref[zi // 2, :, pl.ds(pl.multiple_of(lax.rem(zi, 2) * 256, 256), 256)]

    seen = set()

    def rows_of(f, route, kind, zi):
        buf = bufs[f, route]
        return [buf[kind, zi, core, yi] for yi in range(4) for core in range(2)]

    def column(route, zi):
        cut = SPLIT["u"]
        lanes = pl.ds(0, cut) if route == "a" else pl.ds(cut, FFT - cut)
        for kind in range(2):
            term = dot(y_col(zi), jnp.concatenate(rows_of("u", route, kind, zi), axis=0))
            if (route, kind) in seen:
                acc[kind, :, lanes] += term
            else:
                acc[kind, :, lanes] = term
            seen.add((route, kind))

    for kind, *rest in STEPS["rest"]:
        if kind == "fb":
            net.column_b(*rest)
            column("b", net.zi[rest[1]])
        elif kind == "fa":
            net.column_a(*rest)
            column("a", net.zk(rest[1]))
        elif kind == "hid":
            gate = acc[0] * scale_in
            hid[...] = (gate / (1.0 + jnp.exp(-gate)) * (acc[1] * scale_in)).astype(bf16)
        elif kind == "dn":
            net.column_b("d", COLUMNS.index(rest[1]))
            net.column_a("d", rest[1])
            zi = net.zk(rest[1])
            at = zi // 2
            cut = SPLIT["d"]
            term = jnp.zeros((TOK, 256), f32)
            for route, lanes in (("a", pl.ds(0, cut)), ("b", pl.ds(cut, FFT - cut))):
                rows_d = jnp.concatenate(rows_of("d", route, 0, zi), axis=0)
                term = term + dot(hid[:, lanes], rows_d, ((1,), (1,)))
            part2[zi] = term.astype(bf16)

            @pl.when(at != tp)
            def _():
                copy_to(
                    part2.at[zi],
                    rpart2.at[tp, lax.rem(zi, 2)],
                    ss.at[9],
                    rs.at[9],
                    {"sp": sp, "tp": at},
                ).start()
        else:
            getattr(net, kind)(*rest)
    joint(9, rpart2.at[pl.ds(0, NX - 1)]).wait_recv()
    for half in range(2):
        lanes = slice(256 * half, 256 * half + 256)
        total = resid_f[:, lanes] + part2[2 * tp + half].astype(f32)
        for r in range(1, NX):
            total = total + rpart2[xfrom[r], half].astype(f32)
        o_ref[:, lanes] = total.astype(bf16)
    for n, ref in enumerate(
        (
            small1.at[pl.ds(0, NG - 1)],
            r1.at[pl.ds(0, NG - 1)],
            small2.at[pl.ds(0, NZ - 1)],
            None,
            r3.at[pl.ds(0, NG - 1)],
            rsq.at[0, pl.ds(0, NX - 1)],
            rpart.at[pl.ds(0, NX - 1)],
            rsq.at[1, pl.ds(0, NX - 1)],
            y_ref.at[pl.ds(0, NX - 1)],
            rpart2.at[pl.ds(0, NX - 1)],
        )
    ):
        if ref is not None:
            joint(n, ref).wait_send()
    for r in range(1, NZ):

        @pl.when(z + r < NZ)
        def _(r=r):
            joint(10 + r, r2.at[0]).wait_send()

    net.drain()


def local(
    stream,
    queries,
    keys,
    values,
    out_gate,
    input_gate,
    forget_gate,
    head_gain,
    w_out,
    ffn_gain,
    w_gate,
    w_up,
    w_down,
):
    vmem = pl.BlockSpec(memory_space=pltpu.VMEM)
    hbm = pl.BlockSpec(memory_space=pl.ANY)
    return pl.pallas_call(
        layer_kernel,
        out_shape=pltpu.VMEM((TOK, COLS), bf16),
        in_specs=[hbm] * 13,
        out_specs=vmem,
        scratch_shapes=[
            pltpu.VMEM((2, NZ, 2, 4, 32, SPLIT["u"]), bf16),
            pltpu.VMEM((2, NZ, 2, 4, 32, FFT - SPLIT["u"]), bf16),
            pltpu.VMEM((1, NZ, 2, 4, 32, SPLIT["d"]), bf16),
            pltpu.VMEM((1, NZ, 2, 4, 32, FFT - SPLIT["d"]), bf16),
            pltpu.VMEM((TOK, 2 * DQK), bf16),
            pltpu.VMEM((TOK, 2 * DQK), bf16),
            pltpu.VMEM((TOK, COLS), bf16),
            pltpu.VMEM((TOK, COLS), bf16),
            pltpu.VMEM((2, TOK), f32),
            pltpu.VMEM((2, TOK), f32),
            pltpu.VMEM((1, COLS), f32),
            pltpu.VMEM((COLS, D), bf16),
            pltpu.VMEM((TOK, COLS), bf16),
            pltpu.VMEM((1, D), f32),
            pltpu.VMEM((2, TOK, FFT), f32),
            pltpu.VMEM((TOK, FFT), bf16),
            pltpu.VMEM((NX, TOK, COLS), bf16),
            pltpu.VMEM((NG, 8, TOK), f32),
            pltpu.VMEM((NZ, 8, TOK), f32),
            pltpu.VMEM((NG, 8, TOK), f32),
            pltpu.VMEM((8, TOK), f32),
            pltpu.VMEM((8, TOK), f32),
            pltpu.VMEM((NG, 32, DV), bf16),
            pltpu.VMEM((NG, 32, DV), bf16),
            pltpu.VMEM((NG, 32, DV), f32),
            pltpu.VMEM((32, DV), bf16),
            pltpu.VMEM((NZ, 32, DV), bf16),
            pltpu.VMEM((NG, 32, DV), bf16),
            pltpu.VMEM((NG, 32, DV), bf16),
            pltpu.VMEM((NX, TOK, COLS), bf16),
            pltpu.VMEM((NX, TOK, COLS), bf16),
            pltpu.VMEM((2, 8, TOK), f32),
            pltpu.VMEM((2, NX, 8, TOK), f32),
            pltpu.VMEM((TOK, COLS), bf16),
            pltpu.VMEM((NZ, TOK, 256), bf16),
            pltpu.VMEM((NX, 2, TOK, 256), bf16),
            pltpu.SemaphoreType.DMA((16,)),
            pltpu.SemaphoreType.DMA((18,)),
            pltpu.SemaphoreType.DMA((18,)),
            pltpu.SemaphoreType.DMA((5 * RING,)),
            pltpu.SemaphoreType.DMA((84,)),
        ],
        compiler_params=pltpu.CompilerParams(
            collective_id=0, has_side_effects=True, vmem_limit_bytes=60 * 2**20
        ),
    )(
        queries,
        keys,
        values,
        out_gate,
        input_gate.T,
        forget_gate.T,
        head_gain.reshape(1, COLS),
        w_out,
        stream,
        ffn_gain.reshape(1, D),
        w_gate,
        w_up,
        w_down.T,
    )


def solution(mesh):
    in_specs = (
        P("sp", "tp"),
        P("sp", "tp"),
        P("sp", "tp"),
        P("sp", "tp"),
        P("sp", "tp"),
        P("sp", "tp"),
        P("sp", "tp"),
        P("tp"),
        P("tp", None),
        P(),
        P("sp", "tp"),
        P("sp", "tp"),
        P("tp", "sp"),
    )
    return jax.shard_map(
        local, mesh=mesh, in_specs=in_specs, out_specs=P("sp", "tp"), check_vma=False
    )
```
